32 devices in a mesh: sp: 8 (over z, core), tp: 4 (over y, x).
Axes of the slice: x: 2, y: 2, z: 4, core: 2. Of those that a mesh axis runs over, the one named last changes fastest.
Arguments:
- query_heads: bfloat16 [2048, 1024], P('sp', 'tp'), may hold values from -6 to 6
- key_heads: bfloat16 [2048, 256], P('sp'), may hold values from -6 to 6
- value_heads: bfloat16 [2048, 256], P('sp'), may hold values from -24 to 24
- q_gain: float32 [64], replicated, may hold values from 0.6 to 4.5
- k_gain: float32 [64], replicated, may hold values from 0.6 to 4.5
- out_weight: bfloat16 [1024, 2048], P('tp'), may hold values from -0.1875 to 0.1875
- residual: bfloat16 [2048, 2048], P('sp', 'tp'), may hold values from -3 to 3
- norm_gain: float32 [2048], P('tp'), may hold values from 0.1 to 1.9
- routes: int32 [2048, 2], P('sp'), may hold values from 0 to 7, all different within a row; in each aligned block of 256 rows (0 to 255, 256 to 511, ...) at most 81 rows name the same one
- route_weights: float32 [2048, 2], P('sp'), may hold values from 0.5 to 1.5
- w_gate: bfloat16 [8, 2048, 4096], P('sp', None, 'tp'), may hold values from -0.125 to 0.125
- w_up: bfloat16 [8, 2048, 4096], P('sp', None, 'tp'), may hold values from -0.125 to 0.125
- w_down: bfloat16 [8, 4096, 2048], P('sp', 'tp'), may hold values from -0.1875 to 0.1875
Outputs:
- layer_out: bfloat16 [2048, 2048], P('sp', 'tp')
The draws below stay inside these ranges and needn't reach their ends.
Inputs may be any that keep to these rules, and one draw needn't show every extreme that they name: `routes`: each row names 2 different experts. Among the 256 rows of one index of sp, no expert is named more than 81 times, a bound that some block reaches.
All inputs are finite; a program needn't handle non-finite values.
Results may differ from the reference program's by a relative error of at most 0.02.
The reference program's roundings to bfloat16 on the way count: a program that leaves them out, or rounds other values in their place, can miss the bound.
Values may be sent and summed in bfloat16 or wider, within the bound.
A program may use at most 64 MiB of HBM per device.

```python
import math
import jax
import jax.numpy as jnp
import numpy as np
from jax import lax

D = 2048
HQ = 16
KV = 4
E = 64
FF = 4096
TOPK = 2
GRID_W = 64
TOK_SP = 256
TOKENS = 2048
EXPERTS = 8
CAP = 81
N_SP = 8
N_TP = 4


def base_keys(key):
    drawn = jax.random.normal(jax.random.fold_in(key, 11), (TOKENS, KV * E), jnp.float32)
    return jnp.clip(drawn, -6.0, 6.0)


def draw_key_heads(key, part):
    return base_keys(key).astype(jnp.bfloat16)


def draw_query_heads(key, part):
    fresh = jax.random.normal(jax.random.fold_in(key, 23), (TOKENS, KV, HQ // KV, E), jnp.float32)
    fresh = jnp.clip(fresh, -6.0, 6.0)
    return fresh.reshape(TOKENS, HQ * E).astype(jnp.bfloat16)


def gain_of(key, salt):
    return 1.0 + 0.18 * jax.random.uniform(jax.random.fold_in(key, salt), (E,), jnp.float32, -2.0, 2.0)


def draw_q_gain(key, part):
    return gain_of(key, 31)


def draw_k_gain(key, part):
    return gain_of(key, 37)


def draw_residual(key, part):
    noise_key = jax.random.fold_in(key, 41)
    row_key = jax.random.fold_in(key, 43)
    column_pos = jnp.arange(D, dtype=jnp.float32) / D
    row_scale = jnp.exp(jax.random.uniform(row_key, (TOKENS, 1), jnp.float32, 0.0, jnp.log(2.0)))
    base = jax.random.normal(noise_key, (TOKENS, D), jnp.float32)
    column_scale = 0.05 * jnp.exp(jnp.log(10.0) * column_pos)
    values = base * row_scale * column_scale[None, :]
    return jnp.clip(values, -3.0, 3.0).astype(jnp.bfloat16)


def steps_of(rng, dims, shards, smallest, top_value):
    level = 1.0
    for axis_at, shards_of in shards:
        steps = jax.random.uniform(jax.random.fold_in(jax.random.fold_in(rng, 6), axis_at), (shards_of,), jnp.float32, smallest / len(shards), top_value / len(shards))
        level = level * jnp.repeat(jnp.exp(steps), dims[axis_at] // shards_of).reshape((-1,) + (1,) * (len(dims) - 1 - axis_at))
    return level


def deal_out(key, own, number, rows, count, top, most, slope):
    order = jax.random.permutation(key, count)
    crowded, common = load_shares(count, rows * top, most, slope, True), load_shares(count, rows * top, most, slope, False)
    places = jnp.arange(count)

    def named(tallies, turn):
        used = int((tallies > 0).sum())
        fixed = max(1, used // 4)
        shifted = fixed + (places - fixed + turn * (used - fixed)) % max(1, count - fixed)
        return jnp.zeros((count,), jnp.int32).at[order[jnp.where(places < fixed, places, shifted)]].set(jnp.asarray(tallies, jnp.int32))

    tallies = jnp.where(number % 4 == 0, named(crowded, number // 4), named(common, number - number // 4 - 1))
    mixed = jax.random.permutation(jax.random.fold_in(own, 3), count)
    giver, receiver = mixed[0:count // 2 * 2:2], mixed[1:count // 2 * 2:2]
    room = jnp.minimum(tallies[giver] - 1, most - tallies[receiver]) // 2
    room = jnp.where((giver == order[0]) | (receiver == order[0]) | (tallies[receiver] == 0), 0, jnp.maximum(room, 0))
    shifted = jax.random.randint(jax.random.fold_in(own, 4), (count // 2,), 0, 1 << 20) % (room + 1)
    tallies = tallies.at[giver].add(-shifted).at[receiver].add(shifted)
    labels = jnp.searchsorted(jnp.cumsum(tallies), jnp.arange(rows * top), side="right").astype(jnp.int32)
    table = labels.reshape(top, rows).T
    table = table[jax.random.permutation(jax.random.fold_in(own, 1), rows)]
    turn = jax.random.randint(jax.random.fold_in(own, 2), (rows, 1), 0, top)
    return jnp.take_along_axis(table, (jnp.arange(top)[None, :] + turn) % top, axis=1)


def load_shares(amount, total, bound, lean, full):
    portions = [(1 << 20) // math.isqrt(rank ** lean) + 1 for rank in range(1, amount + 1)]
    largest = bound if full else min(bound, max(-(-total // amount), total * portions[0] // sum(portions)))
    least = 1 if total - largest >= amount - 1 else 0
    holding, spare = [largest] + [least] * (amount - 1), total - largest - least * (amount - 1)
    while spare > 0:
        movable = [i for i in range(1, amount) if holding[i] < largest] or [i for i in range(1, amount) if holding[i] < bound]
        mass, remaining = sum([portions[i] for i in movable]), spare
        for i in movable:
            addition = min(bound - holding[i], max(1, remaining * portions[i] // mass), spare)
            holding[i] = holding[i] + addition
            spare = spare - addition
    return np.array(holding)


def normal_values(stream_key, dims, scale, bound, cuts=(), kind=jnp.bfloat16):
    level = steps_of(stream_key, dims, cuts, -0.22, 0.18) if cuts else 1.0
    array = jax.random.normal(stream_key, dims, jnp.float32) * scale * level
    return jnp.minimum(jnp.maximum(array, -bound), bound).astype(kind)


def setup_inputs(seed: int = 0) -> dict:
    arg_keys = jax.random.split(jax.random.key(seed), 14)
    query_heads = draw_query_heads(jax.random.fold_in(arg_keys[13], 71), 0)
    key_heads = draw_key_heads(jax.random.fold_in(arg_keys[13], 71), 0)
    value_heads = normal_values(arg_keys[2], (TOKENS, KV * E), 4.0, 24.0, ((0, 8),))
    q_gain = draw_q_gain(jax.random.fold_in(arg_keys[13], 71), 0)
    k_gain = draw_k_gain(jax.random.fold_in(arg_keys[13], 71), 0)
    out_weight = normal_values(arg_keys[5], (HQ * E, D), (HQ * E) ** -0.5, 0.1875, ((0, 4),))
    residual = draw_residual(jax.random.fold_in(arg_keys[13], 71), 0)
    norm_gain = jnp.clip(1.0 + 0.18 * jax.random.normal(arg_keys[7], (D,), jnp.float32), 0.1, 1.9)
    routes_keys = jax.random.split(jax.random.fold_in(arg_keys[8], 1), TOKENS // TOK_SP)
    routes_turns = jax.random.permutation(jax.random.fold_in(arg_keys[8], 3), TOKENS // TOK_SP)
    routes = jax.vmap(lambda own, number: deal_out(jax.random.fold_in(arg_keys[8], 2), own, number, TOK_SP, EXPERTS, TOPK, CAP, 1))(routes_keys, routes_turns).reshape((TOKENS, TOPK))
    route_weights = jnp.clip(0.5 + 1.0 * jax.random.uniform(arg_keys[9], (TOKENS, TOPK), jnp.float32) ** steps_of(arg_keys[9], (TOKENS, TOPK), ((0, 8),), -0.2, 0.2), 0.5, 1.5)
    w_gate = normal_values(arg_keys[10], (EXPERTS, D, FF), D ** -0.5, 0.125, ((0, 8), (2, 4)))
    w_up = normal_values(arg_keys[11], (EXPERTS, D, FF), D ** -0.5, 0.125, ((0, 8), (2, 4)))
    w_down = normal_values(arg_keys[12], (EXPERTS, FF, D), (FF // 4) ** -0.5, 0.1875, ((0, 8), (1, 4)))
    return {"query_heads": query_heads, "key_heads": key_heads, "value_heads": value_heads, "q_gain": q_gain, "k_gain": k_gain, "out_weight": out_weight, "residual": residual, "norm_gain": norm_gain, "routes": routes, "route_weights": route_weights, "w_gate": w_gate, "w_up": w_up, "w_down": w_down}


norm_eps = 1e-06
rope_base = 10000.0

def normalize(values_f, gain):
    mean_sq = lax.optimization_barrier(jnp.mean(values_f * values_f, axis=-1, keepdims=True))
    return values_f * lax.rsqrt(mean_sq + norm_eps) * gain

def rotate(values_f, positions):
    head_width = values_f.shape[-1]
    half_width = head_width // 2
    quarter_width = half_width // 2
    frequency = rope_base ** (-jnp.arange(quarter_width, dtype=jnp.float32) / quarter_width)
    grid_rows = (positions // GRID_W).astype(jnp.float32)
    grid_cols = (positions % GRID_W).astype(jnp.float32)
    shape = (values_f.shape[0],) + (1,) * (values_f.ndim - 2) + (quarter_width,)
    pieces = []
    for coords, offset_lo in ((grid_rows, 0), (grid_cols, half_width)):
        angles = coords[:, None] * frequency[None, :]
        cosine = jnp.cos(angles).reshape(shape)
        sines = jnp.sin(angles).reshape(shape)
        first_part = values_f[..., offset_lo:offset_lo + quarter_width]
        second_part = values_f[..., offset_lo + quarter_width:offset_lo + half_width]
        pieces.append(first_part * cosine - second_part * sines)
        pieces.append(second_part * cosine + first_part * sines)
    return jnp.concatenate(pieces, axis=-1)

def slots_of(assign):
    onehot = (assign[:, None] == jnp.arange(EXPERTS, dtype=jnp.int32)[None, :]).astype(jnp.int32)
    before = jnp.cumsum(onehot, axis=0) - onehot
    return lax.optimization_barrier(jnp.sum(before * onehot, axis=1)).astype(jnp.int32)

def reference(query_heads, key_heads, value_heads, q_gain, k_gain, out_weight, residual, norm_gain, routes, route_weights, w_gate, w_up, w_down):
    group_size = HQ // KV
    positions = jnp.arange(TOKENS, dtype=jnp.int32)
    query_f = query_heads.astype(jnp.float32).reshape(TOKENS, KV, group_size, E)
    q_turned = rotate(normalize(query_f, q_gain), positions).astype(jnp.bfloat16)
    key_f = key_heads.astype(jnp.float32).reshape(TOKENS, KV, E)
    k_turned = rotate(normalize(key_f, k_gain), positions).astype(jnp.bfloat16).astype(jnp.float32)
    value_f = value_heads.astype(jnp.float32).reshape(TOKENS, KV, E)

    def query_block(block_q):
        scores = jnp.einsum('qcge,kce->cgqk', block_q.astype(jnp.float32), k_turned) * E ** (-0.5)
        row_max = lax.optimization_barrier(jnp.max(scores, axis=-1, keepdims=True))
        exped = jnp.exp(scores - row_max)
        denominator = lax.optimization_barrier(jnp.sum(exped, axis=-1))
        rounded = lax.optimization_barrier(exped.astype(jnp.bfloat16))
        weighted = jnp.einsum('cgqk,kce->qcge', rounded.astype(jnp.float32), value_f)
        return (weighted / jnp.transpose(denominator, (2, 0, 1))[..., None]).astype(jnp.bfloat16)
    attended = lax.map(query_block, q_turned.reshape(N_SP, TOK_SP, KV, group_size, E))
    attended = attended.reshape(TOKENS, HQ * E)
    rows_tp = HQ * E // N_TP
    head_blocks = attended.reshape(TOKENS, N_TP, rows_tp).transpose(1, 0, 2)
    weight_blocks = out_weight.reshape(N_TP, rows_tp, D)

    def add_block(running, operands):
        partial_value = jnp.dot(operands[0], operands[1], preferred_element_type=jnp.float32).astype(jnp.bfloat16)
        partial_value = lax.optimization_barrier(partial_value)
        return (running + partial_value.astype(jnp.float32), None)
    attn_out, _ = lax.scan(add_block, jnp.zeros((TOKENS, D), jnp.float32), (head_blocks, weight_blocks))
    after_attn = residual.astype(jnp.float32) + attn_out
    mean_sq = lax.optimization_barrier(jnp.mean(after_attn * after_attn, axis=1, keepdims=True))
    normed = (after_attn * lax.rsqrt(mean_sq + norm_eps) * norm_gain).astype(jnp.bfloat16)
    assign = routes.reshape(N_SP, TOK_SP * TOPK)
    slot_rank = jax.vmap(slots_of)(assign)
    slot_index = assign * CAP + slot_rank
    token_local = (jnp.arange(TOK_SP * TOPK, dtype=jnp.int32) // TOPK).astype(jnp.int32)

    def table_of(indices):
        return jnp.full((EXPERTS * CAP,), TOK_SP, jnp.int32).at[indices].set(token_local)
    slot_token = jax.vmap(table_of)(slot_index)
    group_start = (jnp.arange(N_SP, dtype=jnp.int32) * TOK_SP)[:, None]
    global_token = jnp.where(slot_token < TOK_SP, slot_token + group_start, TOKENS).astype(jnp.int32)
    row_index = global_token.reshape(N_SP, EXPERTS, CAP).transpose(1, 0, 2).reshape(EXPERTS, N_SP * CAP)
    padded = jnp.concatenate([normed, jnp.zeros((1, D), jnp.bfloat16)], axis=0)
    hidden_tp = FF // N_TP

    def expert(operands):
        indices, gate_w, up_w, down_w = operands
        gathered = padded[indices]
        gate_sum = jnp.dot(gathered, gate_w, preferred_element_type=jnp.float32)
        up_sum = jnp.dot(gathered, up_w, preferred_element_type=jnp.float32)
        activated = (jax.nn.silu(gate_sum) * up_sum).astype(jnp.bfloat16)
        act_blocks = activated.reshape(N_SP * CAP, N_TP, hidden_tp).transpose(1, 0, 2)
        down_blocks = down_w.reshape(N_TP, hidden_tp, D)

        def add_part(running, pair):
            partial_value = jnp.dot(pair[0], pair[1], preferred_element_type=jnp.float32).astype(jnp.bfloat16)
            partial_value = lax.optimization_barrier(partial_value)
            return (running + partial_value.astype(jnp.float32), None)
        total, _ = lax.scan(add_part, jnp.zeros((N_SP * CAP, D), jnp.float32), (act_blocks, down_blocks))
        return total.astype(jnp.bfloat16)
    expert_rows = lax.map(expert, (row_index, w_gate, w_up, w_down)).reshape(EXPERTS, N_SP, CAP, D)
    group_idx = jnp.arange(N_SP, dtype=jnp.int32)[:, None]
    picked = expert_rows[assign, group_idx, slot_rank].astype(jnp.float32)
    picked = picked.reshape(TOKENS, TOPK, D)
    expert_mix = lax.optimization_barrier(jnp.sum(picked * route_weights[:, :, None], axis=1))
    return (after_attn + expert_mix).astype(jnp.bfloat16)
```

```python
import functools

import jax
import jax.numpy as jnp
import numpy as np
from jax import lax
from jax.experimental import pallas as pl
from jax.experimental.pallas import tpu as pltpu
from jax.sharding import PartitionSpec as P

D = 2048
HQ = 16
KV = 4
E = 64
TOPK = 2
GRID_W = 64

norm_eps = 1e-06
rope_base = 10000.0

MESH = pl.DeviceIdType.MESH
VMEM = pltpu.VMEM
F32 = jnp.float32
BF16 = jnp.bfloat16
ROW_TILE = 8


def normalize(values_f, gain):
    mean_sq = jnp.mean(values_f * values_f, axis=-1, keepdims=True)
    return values_f * lax.rsqrt(mean_sq + norm_eps) * gain


def rotate(values_f, positions):
    head_width = values_f.shape[-1]
    half_width = head_width // 2
    quarter_width = half_width // 2
    frequency = rope_base ** (-jnp.arange(quarter_width, dtype=jnp.float32) / quarter_width)
    grid_rows = (positions // GRID_W).astype(jnp.float32)
    grid_cols = (positions % GRID_W).astype(jnp.float32)
    shape = (values_f.shape[0],) + (1,) * (values_f.ndim - 2) + (quarter_width,)
    pieces = []
    for coords, offset_lo in ((grid_rows, 0), (grid_cols, half_width)):
        angles = coords[:, None] * frequency[None, :]
        cosine = jnp.cos(angles).reshape(shape)
        sines = jnp.sin(angles).reshape(shape)
        first_part = values_f[..., offset_lo : offset_lo + quarter_width]
        second_part = values_f[..., offset_lo + quarter_width : offset_lo + half_width]
        pieces.append(first_part * cosine - second_part * sines)
        pieces.append(second_part * cosine + first_part * sines)
    return jnp.concatenate(pieces, axis=-1)


def dot(a, b):
    return jnp.dot(a, b, preferred_element_type=F32)


def tp_offset(tp, n_tp, q):
    if n_tp == 4:
        x = lax.rem(lax.rem(tp, 2) + q % 2, 2)
        y = lax.rem(lax.div(tp, 2) + q // 2, 2)
        return y * 2 + x
    return lax.rem(tp + q, n_tp)


def tp_origin(tp, n_tp, q):
    return tp_offset(tp, n_tp, q if n_tp == 4 else n_tp - q)


def remote(src, dst, send_sem, recv_sem, sp, tp):
    return pltpu.make_async_remote_copy(
        src_ref=src, dst_ref=dst, send_sem=send_sem, recv_sem=recv_sem,
        device_id=(sp, tp), device_id_type=MESH,
    )


def gather_kernel(
    n_sp, n_tp, own, weight, out, weight_out, send, recv, send2, recv2, w_send, w_recv,
    v_send, v_recv
):
    me = lax.axis_index("sp")
    tp = lax.axis_index("tp")
    chips = n_sp // 2
    core = lax.rem(me, 2)
    z = lax.div(me, 2)
    partner = z * 2 + 1 - core
    barrier = pltpu.get_barrier_semaphore()
    pl.semaphore_signal(barrier, inc=1, device_id=(partner, tp), device_id_type=MESH)
    for j in range(1, chips):
        pl.semaphore_signal(
            barrier, inc=1, device_id=(lax.rem(z + j, chips) * 2 + core, tp), device_id_type=MESH
        )
    for q in range(1, n_tp):
        pl.semaphore_signal(
            barrier, inc=1, device_id=(me, tp_offset(tp, n_tp, q)), device_id_type=MESH
        )
    pl.semaphore_wait(barrier, chips + n_tp - 1)
    first = []
    for j in range(1, chips):
        copy = remote(own, out.at[me], send.at[j], recv.at[j], lax.rem(z + j, chips) * 2 + core, tp)
        copy.start()
        first.append(copy)
    swap = remote(own, out.at[me], send2.at[0], recv2.at[0], partner, tp)
    swap.start()
    out[me] = own[...]
    cols = weight_out.shape[2]
    depth = weight.shape[0] // 2
    mine = pl.ds(pl.multiple_of(core * depth, 16), depth)
    third = {}
    for q in range(n_tp - 1, 0, -1):
        peer = tp_offset(tp, n_tp, q)
        part = weight.at[mine, pl.ds(pl.multiple_of(peer * cols, 128), cols)]
        third[q] = remote(
            part, weight_out.at[tp, mine, :], w_send.at[q], w_recv.at[q], me, peer
        )
        third[q].start()
    weight_out[tp] = weight[:, pl.ds(pl.multiple_of(tp * cols, 128), cols)]
    second = [swap]
    for j in range(1, chips):
        first[j - 1].wait_recv()
        source = lax.rem(z + chips - j, chips) * 2 + core
        copy = remote(out.at[source], out.at[source], send2.at[j], recv2.at[j], partner, tp)
        copy.start()
        second.append(copy)
    for q in range(1, n_tp):
        third[q].wait_recv()
        part = weight_out.at[tp_origin(tp, n_tp, q), mine, :]
        copy = remote(part, part, v_send.at[q], v_recv.at[q], partner, tp)
        copy.start()
        second.append(copy)
    for copy in second:
        copy.wait()
    for copy in first + list(third.values()):
        copy.wait_send()


def gather_kv(n_sp, n_tp, own, weight):
    rows, width = own.shape
    depth, feats = weight.shape
    return pl.pallas_call(
        functools.partial(gather_kernel, n_sp, n_tp),
        out_shape=(
            jax.ShapeDtypeStruct((n_sp, rows, width), own.dtype),
            jax.ShapeDtypeStruct((n_tp, depth, feats // n_tp), weight.dtype),
        ),
        in_specs=[pl.BlockSpec(memory_space=VMEM)] * 2,
        out_specs=[pl.BlockSpec(memory_space=VMEM)] * 2,
        scratch_shapes=[pltpu.SemaphoreType.DMA((n_sp // 2,))] * 4
        + [pltpu.SemaphoreType.DMA((n_tp,))] * 4,
        compiler_params=pltpu.CompilerParams(collective_id=0, has_side_effects=True),
    )(own, weight)


def layer_kernel(
    n_sp, n_tp, capacity, groups,
    attended, out_weight, residual, gain, routes, routes_t, mix_w, w_gate, w_up, w_down,
    out,
    wg, wu, wd, p_in, after, n_out, n_in, x_out, x_all, act, y_out, y_in, y_own, y_keep, y_fwd, y_last,
    z_out, z_in,
    w_sem, p_send, p_recv, n_send, n_recv, x_send, x_recv, a_send, a_recv, r_send, r_recv,
    y_send, y_recv, e_send, e_recv, z_send, z_recv,
):
    me = lax.axis_index("sp")
    tp = lax.axis_index("tp")
    rows, cols = residual.shape
    hidden = w_gate.shape[1]
    square = n_tp == 4

    def to_tp(q):
        return tp_offset(tp, n_tp, q)

    def from_tp(q):
        return tp_origin(tp, n_tp, q)

    def to_sp(j):
        return lax.rem(me + j, n_sp)

    def from_sp(j):
        return lax.rem(me + n_sp - j, n_sp)

    def feats(t, width=cols, shift=0):
        return pl.ds(pl.multiple_of(t * cols + shift, 128), width)

    def block(j):
        return pl.ds(j * capacity, capacity)

    loads = [
        pltpu.make_async_copy(s, d, w_sem.at[i])
        for i, (s, d) in enumerate(((w_gate, wg), (w_up, wu), (w_down, wd)))
    ]
    for load in loads:
        load.start()

    barrier = pltpu.get_barrier_semaphore()
    for q in range(1, n_tp):
        pl.semaphore_signal(barrier, inc=1, device_id=(me, to_tp(q)), device_id_type=MESH)
    for j in range(1, n_sp):
        pl.semaphore_signal(barrier, inc=1, device_id=(to_sp(j), tp), device_id_type=MESH)
    pl.semaphore_wait(barrier, n_tp - 1 + n_sp - 1)

    order = [3, 1, 2] if square else list(range(1, n_tp))
    p_copies = {}
    for q in order:
        p_copies[q] = remote(attended, p_in.at[q], p_send.at[q], p_recv.at[q], me, to_tp(q))
        p_copies[q].start()
    total = dot(attended[...], out_weight[tp]).astype(BF16).astype(F32)

    tri = lax.broadcasted_iota(jnp.int32, (rows, rows), 0)
    tri_c = lax.broadcasted_iota(jnp.int32, (rows, rows), 1)
    upper = (tri < tri_c).astype(F32).astype(BF16)
    lower = (tri > tri_c).astype(F32).astype(BF16)
    expert_rows = lax.broadcasted_iota(jnp.int32, (n_sp, rows), 0)
    expert_cols = lax.broadcasted_iota(jnp.int32, (rows, n_sp), 1)
    hot_r = [(routes_t[k : k + 1, :] == expert_rows).astype(F32) for k in range(TOPK)]
    hot_c = [(routes[:, k : k + 1] == expert_cols).astype(F32) for k in range(TOPK)]
    before_r = dot(sum(hot_r).astype(BF16), upper)
    before_c = dot(lower, sum(hot_c).astype(BF16))
    slot_r, slot_c = [], []
    for k in range(TOPK):
        rank = jnp.sum(before_r * hot_r[k], axis=0, keepdims=True).astype(jnp.int32)
        rel = routes_t[k : k + 1, :] - me
        rel = jnp.where(rel < 0, rel + n_sp, rel)
        slot_r.append(rel * capacity + rank)
        rank = jnp.sum(before_c * hot_c[k], axis=1, keepdims=True).astype(jnp.int32)
        rel = routes[:, k : k + 1] - me
        rel = jnp.where(rel < 0, rel + n_sp, rel)
        slot_c.append(rel * capacity + rank)

    total = residual[...].astype(F32) + total
    for q in [1, 2, 3] if square else order:
        p_copies[q].wait_recv()
        total = total + dot(p_in[q], out_weight[from_tp(q)]).astype(BF16).astype(F32)
    after[...] = total
    square_sum = jnp.sum(total * total, axis=1, keepdims=True)
    as_rows = jnp.transpose(jnp.broadcast_to(square_sum, (rows, 128)))
    n_out[...] = as_rows[0:8, :]
    n_copies = []
    for q in range(1, n_tp):
        copy = remote(n_out, n_in.at[q], n_send.at[q], n_recv.at[q], me, to_tp(q))
        copy.start()
        n_copies.append(copy)
    sum_rows = n_out[...]
    for q in range(1, n_tp):
        n_copies[q - 1].wait_recv()
        sum_rows = sum_rows + n_in[q]
    all_sum = jnp.transpose(jnp.broadcast_to(sum_rows[0:1, :], (128, rows)))[:, 0:1]
    normed = (after[...] * lax.rsqrt(all_sum / D + norm_eps) * gain[...]).astype(BF16)

    x_copies = {}
    slot_id = lax.broadcasted_iota(jnp.int32, (capacity, rows), 0)
    for j in list(range(1, n_sp)) + [0]:
        ids = slot_id + j * capacity
        pick = ((ids == slot_r[0]) | (ids == slot_r[1])).astype(F32).astype(BF16)
        picked = dot(pick, normed).astype(BF16)
        x_out[j] = picked
        if j:
            x_copies[j] = remote(
                x_out.at[j], x_all.at[block(j), feats(tp)], x_send.at[j], x_recv.at[j], to_sp(j), tp
            )
            x_copies[j].start()
        else:
            x_all[block(0), feats(tp)] = picked

    direct = [1, 2] if square else list(range(1, n_tp))
    a_copies, r_copies = {}, {}

    def spread(j):
        if j:
            x_copies[j].wait_recv()
        part = x_all.at[block(j), feats(tp)]
        for q in direct:
            a_copies[q, j] = remote(part, part, a_send.at[q, j], a_recv.at[q, j], me, to_tp(q))
            a_copies[q, j].start()

    def await_direct(q, j):
        part = x_all.at[block(j), feats(from_tp(q))]
        remote(part, part, a_send.at[q, j], a_recv.at[q, j], me, to_tp(q)).wait_recv()

    def relay(j):
        half = cols // 2
        for i, q in enumerate((1, 2)):
            await_direct(q, j)
            part = x_all.at[block(j), feats(to_tp(q), half, i * half)]
            r_copies[i, j] = remote(part, part, r_send.at[i, j], r_recv.at[i, j], me, to_tp(3 - q))
            r_copies[i, j].start()

    def await_block(j):
        if square:
            half = cols // 2
            for i in range(2):
                part = x_all.at[block(j), feats(to_tp(3), half, i * half)]
                remote(part, part, r_send.at[i, j], r_recv.at[i, j], me, tp_peer).wait_recv()
        else:
            for q in direct:
                await_direct(q, j)

    tp_peer = to_tp(1)
    lag = 2
    for j in range(n_sp + lag):
        if j < n_sp:
            spread(j)
        if square and j >= lag:
            relay(j - lag)

    for load in loads:
        load.wait()
    per = n_sp // groups
    m = per * capacity
    tile = min(256, hidden)
    y_copies, e_copies, z_copies = {}, {}, {}
    half = cols // 2

    def send_parts(j):
        for i in range(2):
            at = (i, slice(None), block(j), slice(None))
            y_copies[i, j] = remote(
                y_out.at[at], y_in.at[at], y_send.at[i, j], y_recv.at[i, j], me, to_tp(1 + i)
            )
            y_copies[i, j].start()

    def pass_on(j):
        for i in range(2):
            y_copies[i, j].wait_recv()
            both = y_in[i, 0, block(j), :].astype(F32) + y_keep[i, block(j), :].astype(F32)
            y_fwd[i, block(j), :] = both.astype(BF16)
            at = (i, block(j), slice(None))
            e_copies[i, j] = remote(
                y_fwd.at[at], y_last.at[at], e_send.at[i, j], e_recv.at[i, j], me, to_tp(2 - i)
            )
            e_copies[i, j].start()

    def finish(j):
        if square:
            pieces = []
            for i in range(2):
                e_copies[i, j].wait_recv()
                piece = y_own[block(j), i * half : (i + 1) * half].astype(F32)
                piece = piece + y_in[i, 1, block(j), :].astype(F32)
                pieces.append((piece + y_last[i, block(j), :].astype(F32)).astype(BF16))
        else:
            acc = y_own[block(j), :].astype(F32)
            for q in range(1, n_tp):
                y_copies[q, j].wait_recv()
                acc = acc + y_in[q, block(j), :].astype(F32)
            pieces = [acc.astype(BF16)]
        width = cols // len(pieces)
        for i, piece in enumerate(pieces):
            at = slice(i * width, (i + 1) * width)
            if j == 0:
                z_in[0:capacity, at] = piece
            else:
                z_out[j, :, at] = piece
        if j:
            z_copies[j] = remote(
                z_out.at[j], z_in.at[block(j), :], z_send.at[j], z_recv.at[j], from_sp(j), tp
            )
            z_copies[j].start()

    for g in range(groups):
        for b in range(per):
            await_block(g * per + b)
        span = pl.ds(g * m, m)

        def hidden_tile(i, carry):
            at = pl.ds(pl.multiple_of(i * tile, 128), tile)
            gate = dot(x_all[span, :], wg[:, at])
            up = dot(x_all[span, :], wu[:, at])
            act[:, at] = (gate / (1.0 + jnp.exp(-gate)) * up).astype(BF16)
            return carry

        lax.fori_loop(0, hidden // tile, hidden_tile, 0)
        blocks = range(g * per, (g + 1) * per)
        if square:
            diag = dot(act[...], wd[:, feats(to_tp(3))]).astype(BF16)
            y_out[0, 0, span, :] = diag[:, :half]
            y_out[1, 0, span, :] = diag[:, half:]
            by_x = dot(act[...], wd[:, feats(to_tp(1))]).astype(BF16)
            y_out[0, 1, span, :] = by_x[:, :half]
            y_keep[1, span, :] = by_x[:, half:]
            by_y = dot(act[...], wd[:, feats(to_tp(2))]).astype(BF16)
            y_out[1, 1, span, :] = by_y[:, half:]
            y_keep[0, span, :] = by_y[:, :half]
            for j in blocks:
                send_parts(j)
        else:
            for q in order:
                y_out[q, span, :] = dot(act[...], wd[:, feats(to_tp(q))]).astype(BF16)
                for j in blocks:
                    at = (q, block(j), slice(None))
                    y_copies[q, j] = remote(
                        y_out.at[at], y_in.at[at], y_send.at[q, j], y_recv.at[q, j], me, to_tp(q)
                    )
                    y_copies[q, j].start()
        y_own[span, :] = dot(act[...], wd[:, feats(tp)]).astype(BF16)
    for j in range(n_sp + lag):
        if square and j < n_sp:
            pass_on(j)
        if j >= lag:
            finish(j - lag)

    slot_lane = lax.broadcasted_iota(jnp.int32, (rows, n_sp * capacity), 1)
    picks = [(slot_lane == slot_c[k]).astype(F32).astype(BF16) for k in range(TOPK)]
    for j in range(1, n_sp):
        z_copies[j].wait_recv()
    mix = dot(picks[0], z_in[...]) * mix_w[:, 0:1]
    mix = mix + dot(picks[1], z_in[...]) * mix_w[:, 1:2]
    out[...] = (after[...] + mix).astype(BF16)

    for copies in (p_copies, x_copies, a_copies, r_copies, y_copies, e_copies, z_copies):
        for copy in copies.values():
            copy.wait_send()
    for copy in n_copies:
        copy.wait_send()


def layer(
    n_sp, n_tp, attended, out_weight, residual, norm_gain, routes, route_weights,
    w_gate, w_up, w_down,
):
    rows, cols = residual.shape
    hidden = w_gate.shape[1]
    capacity = 5 * rows * TOPK // (4 * n_sp) + 1
    capacity = -(-capacity // ROW_TILE) * ROW_TILE
    groups = 2
    slots = n_sp * capacity
    square = n_tp == 4
    parts = (2, 2, slots, cols // 2) if square else (n_tp, slots, cols)
    relayed = (2, slots, cols // 2) if square else (2, 8, 128)
    dma = pltpu.SemaphoreType.DMA
    vmem = pl.BlockSpec(memory_space=VMEM)
    hbm = pl.BlockSpec(memory_space=pl.ANY)
    return pl.pallas_call(
        functools.partial(layer_kernel, n_sp, n_tp, capacity, groups),
        out_shape=jax.ShapeDtypeStruct((rows, cols), BF16),
        in_specs=[vmem] * 7 + [hbm] * 3,
        out_specs=vmem,
        scratch_shapes=[
            VMEM((D, hidden), BF16),
            VMEM((D, hidden), BF16),
            VMEM((hidden, D), BF16),
            VMEM((n_tp,) + attended.shape, BF16),
            VMEM((rows, cols), F32),
            VMEM((8, rows), F32),
            VMEM((n_tp, 8, rows), F32),
            VMEM((n_sp, capacity, cols), BF16),
            VMEM((slots, D), BF16),
            VMEM((slots // groups, hidden), BF16),
            VMEM(parts, BF16),
            VMEM(parts, BF16),
            VMEM((slots, cols), BF16),
            VMEM(relayed, BF16),
            VMEM(relayed, BF16),
            VMEM(relayed, BF16),
            VMEM((n_sp, capacity, cols), BF16),
            VMEM((slots, cols), BF16),
            dma((3,)),
            dma((n_tp,)), dma((n_tp,)),
            dma((n_tp,)), dma((n_tp,)),
            dma((n_sp,)), dma((n_sp,)),
            dma((n_tp, n_sp)), dma((n_tp, n_sp)),
            dma((2, n_sp)), dma((2, n_sp)),
            dma((n_tp, n_sp)), dma((n_tp, n_sp)),
            dma((2, n_sp)), dma((2, n_sp)),
            dma((n_sp,)), dma((n_sp,)),
        ],
        compiler_params=pltpu.CompilerParams(
            collective_id=1, has_side_effects=True, vmem_limit_bytes=60 * 1024 * 1024
        ),
    )(
        attended, out_weight, residual, norm_gain.reshape(1, cols), routes, routes.T,
        route_weights, w_gate, w_up, w_down,
    )


def shards(
    n_sp,
    n_tp,
    query_heads,
    key_heads,
    value_heads,
    q_gain,
    k_gain,
    out_weight,
    residual,
    norm_gain,
    routes,
    route_weights,
    w_gate,
    w_up,
    w_down,
):
    tok_rows = query_heads.shape[0]
    head_local = query_heads.shape[1] // E
    group_size = HQ // KV
    kv_count = max(head_local // group_size, 1)
    per_kv = head_local // kv_count
    tp_index = lax.axis_index("tp")
    sp_index = lax.axis_index("sp")
    kv_first = tp_index * head_local // group_size
    positions = sp_index * tok_rows + jnp.arange(tok_rows, dtype=jnp.int32)
    query_f = query_heads.astype(jnp.float32).reshape(tok_rows, kv_count, per_kv, E)
    q_turned = rotate(normalize(query_f, q_gain), positions).astype(jnp.bfloat16)
    key_cols = lax.dynamic_slice_in_dim(key_heads, kv_first * E, kv_count * E, 1)
    value_cols = lax.dynamic_slice_in_dim(value_heads, kv_first * E, kv_count * E, 1)
    key_f = key_cols.astype(jnp.float32).reshape(tok_rows, kv_count, E)
    k_turned = rotate(normalize(key_f, k_gain), positions).astype(jnp.bfloat16)
    width = kv_count * E
    own = jnp.concatenate([k_turned.reshape(tok_rows, width), value_cols], axis=1)
    both, out_weight = gather_kv(n_sp, n_tp, own, out_weight)
    both = both.reshape(n_sp * tok_rows, 2 * width)
    key_block = both[:, :width].reshape(-1, kv_count, E)
    value_block = both[:, width:].reshape(-1, kv_count, E)
    scores = jnp.einsum(
        "qcge,kce->cgqk", q_turned, key_block, preferred_element_type=jnp.float32
    ) * E ** (-0.5)
    new_max = jnp.max(scores, axis=-1)
    exped = jnp.exp(scores - new_max[..., None])
    denominator = jnp.sum(exped, axis=-1)
    weighted = jnp.einsum(
        "cgqk,kce->cgqe",
        exped.astype(jnp.bfloat16),
        value_block,
        preferred_element_type=jnp.float32,
    )
    attended = (weighted / denominator[..., None]).astype(jnp.bfloat16)
    attended = attended.transpose(2, 0, 1, 3).reshape(tok_rows, head_local * E)
    return layer(
        n_sp, n_tp, attended, out_weight, residual, norm_gain, routes, route_weights,
        w_gate[0], w_up[0], w_down[0],
    )


def flip(index, bits, size):
    mirrored = 0
    step = 1
    while step < size:
        digit = lax.rem(lax.div(index, step), 2)
        mirrored = mirrored + step * (1 - digit if bits & step else digit)
        step *= 2
    return mirrored


def swap_lanes(lanes, quarter):
    return jnp.where(jnp.bitwise_and(lanes, quarter) == 0, lanes + quarter, lanes - quarter)


def swap_quarters(gain, quarter):
    parts = [gain[:, i * quarter : (i + 1) * quarter] for i in (1, 0, 3, 2)]
    return jnp.concatenate(parts, axis=1)


def as_bf16(mask):
    return mask.astype(F32).astype(BF16)


def square_sums(values_f, same_head):
    squared = values_f * values_f
    high = squared.astype(BF16)
    low = (squared - high.astype(F32)).astype(BF16)
    return dot(high, same_head) + dot(low, same_head)


def fused_kernel(
    n_sp, n_tp, base, tail, chunks, order,
    weight, w_gate, w_up, w_down, *rest,
):
    small, out, staged, rest = rest[:10], rest[10], rest[11:21], rest[21:]
    query, keys, values, q_gain, k_gain, table, residual, gain, routes_t, mix_t = staged
    (
        wg, wu, wd, wo, own, kv, q_st, scores_st, top, probs, denom, att, pick_st, mixers,
        after, n_out, n_in, s_out, s_in, x_out, x_tail, x_all, act,
        y_out, y_in, y_own, y_keep, y_fwd, y_last, z_out, z_tail, z_in,
        l_sem, w_sem, o_send, o_recv, v_send, v_recv, k_send, k_recv, p_send, p_recv,
        n_send, n_recv, s_send, s_recv, x_send, x_recv, g_send, g_recv, a_send, a_recv, r_send, r_recv,
        y_send, y_recv, e_send, e_recv, z_send, z_recv, h_send, h_recv,
    ) = rest
    me = lax.axis_index("sp")
    tp = lax.axis_index("tp")
    rows, cols = out.shape
    hidden = wg.shape[1]
    features = cols * n_tp
    width = query.shape[1]
    heads = width // E
    chunk = rows // chunks
    stacked = heads * chunk
    groups = n_sp // 2
    pair = 2 * base
    extra = -(-n_sp * tail // 8) * 8
    cap = base + extra
    full = n_sp * base
    half = cols // 2
    core = lax.rem(me, 2)
    sp_peer = [flip(me, i, n_sp) for i in range(n_sp)]
    tp_peer = [flip(tp, q, n_tp) for q in range(n_tp)]
    sent = []

    def start(copy):
        copy.start()
        sent.append(copy)
        return copy

    def feats(q, size=cols, shift=0):
        return pl.ds(pl.multiple_of(tp_peer[q] * cols + shift, 128), size)

    def block(i):
        return pl.ds(i * base, base if i < n_sp else extra)

    barrier = pltpu.get_barrier_semaphore()
    for q in range(1, n_tp):
        pl.semaphore_signal(barrier, inc=1, device_id=(me, tp_peer[q]), device_id_type=MESH)
    for i in range(1, n_sp):
        pl.semaphore_signal(barrier, inc=1, device_id=(sp_peer[i], tp), device_id_type=MESH)
    fetches = [
        pltpu.make_async_copy(s, d, l_sem.at[i]) for i, (s, d) in enumerate(zip(small, staged))
    ]
    for i in (1, 2, 4, 5, 0, 3, 8, 9, 6, 7):
        fetches[i].start()
    own_cols = pltpu.make_async_copy(weight.at[:, feats(0)], wo.at[0], w_sem.at[3])
    own_cols.start()

    quarter = E // 4
    kv_first = lax.div(tp * heads * KV, HQ)
    source = lax.broadcasted_iota(jnp.int32, (keys.shape[1], 2 * E), 0) - kv_first * E
    lanes = lax.broadcasted_iota(jnp.int32, (keys.shape[1], 2 * E), 1)
    first = lanes < E
    for i in (1, 2, 4, 5):
        fetches[i].wait()
    k_f = dot(keys[...], as_bf16((source == lanes) & first))
    k_swap = dot(keys[...], as_bf16((source == swap_lanes(lanes, quarter)) & first))
    v_f = dot(values[...], as_bf16((source == lanes - E) & (lanes >= E)))
    grid_rows = rows // GRID_W
    all_rows = table.shape[0] - GRID_W
    by_col = table[all_rows:, :]
    turns = jnp.concatenate(
        [by_col + table[pl.ds(me * grid_rows + j, 1), :] for j in range(grid_rows)], axis=0
    )
    cosine, sine = turns[:, : 2 * E], turns[:, 2 * E :]
    gain_k = jnp.concatenate([k_gain[...]] * 2, axis=1)
    gain_ks = jnp.concatenate([swap_quarters(k_gain[...], quarter)] * 2, axis=1)
    sums = square_sums(k_f, jnp.ones((2 * E, 2 * E), BF16))
    k_turned = (k_f * gain_k) * cosine + (k_swap * gain_ks) * sine
    k_turned = k_turned * lax.rsqrt(sums / E + norm_eps)
    own[...] = (k_turned + v_f).astype(BF16)

    pl.semaphore_wait(barrier, n_tp - 1 + n_sp - 1)

    k_copies = {}
    for g in range(1, groups):
        k_copies[2 * g] = start(
            remote(own, kv.at[2 * g], k_send.at[2 * g], k_recv.at[2 * g], sp_peer[2 * g], tp)
        )
    k_copies[1] = start(remote(own, kv.at[1], k_send.at[1], k_recv.at[1], sp_peer[1], tp))
    depth = wo.shape[1] // 2
    mine = pl.ds(pl.multiple_of(core * depth, 16), depth)
    o_copies = {}
    for q in (3, 1, 2):
        o_copies[q] = start(
            remote(
                weight.at[mine, feats(q)], wo.at[q, mine, :], o_send.at[q], o_recv.at[q],
                me, tp_peer[q],
            )
        )
    loads = [
        pltpu.make_async_copy(s, d, w_sem.at[i])
        for i, (s, d) in enumerate(((w_gate, wg), (w_up, wu), (w_down, wd)))
    ]
    for load in loads:
        load.start()
    kv[0] = own[...]

    for i in (0, 3, 8, 9, 6, 7):
        fetches[i].wait()
    from_lane = lax.broadcasted_iota(jnp.int32, (width, width), 0)
    to_lane = lax.broadcasted_iota(jnp.int32, (width, width), 1)
    head_bits = width - E
    same = as_bf16(
        jnp.bitwise_and(from_lane, head_bits) == jnp.bitwise_and(to_lane, head_bits)
    )
    q_f = query[...].astype(F32)
    q_swap = dot(query[...], as_bf16(from_lane == swap_lanes(to_lane, quarter)))
    copies_of = width // (2 * E)
    gain_q = jnp.concatenate([q_gain[...]] * heads, axis=1)
    gain_qs = jnp.concatenate([swap_quarters(q_gain[...], quarter)] * heads, axis=1)
    q_turned = (q_f * gain_q) * jnp.concatenate([cosine] * copies_of, axis=1)
    q_turned = q_turned + (q_swap * gain_qs) * jnp.concatenate([sine] * copies_of, axis=1)
    q_turned = q_turned * lax.rsqrt(square_sums(q_f, same) / E + norm_eps)
    q_turned = (q_turned * E ** (-0.5)).astype(BF16)
    q_st[...] = jnp.zeros_like(q_st)
    for c in range(chunks):
        for h in range(heads):
            q_st[pl.ds((c * heads + h) * chunk, chunk), 0:E] = q_turned[
                c * chunk : (c + 1) * chunk, h * E : (h + 1) * E
            ]

    def score(i):
        at = pl.ds(i * rows, rows)

        def score_chunk(c, carry):
            span = pl.ds(pl.multiple_of(c * stacked, 16), stacked)
            s = lax.dot_general(
                q_st[span, :], kv[i], (((1,), (1,)), ((), ())), preferred_element_type=F32
            )
            scores_st[span, at] = s
            folded = s[:, 0:128]
            for lane in range(128, rows, 128):
                folded = jnp.maximum(folded, s[:, lane : lane + 128])
            top[span, :] = folded if i == 0 else jnp.maximum(top[span, :], folded)
            return carry

        lax.fori_loop(0, chunks, score_chunk, 0)

    def pass_kv(g):
        k_copies[2 * g].wait_recv()
        k_copies[2 * g + 1] = start(
            remote(
                kv.at[2 * g], kv.at[2 * g + 1], k_send.at[2 * g + 1], k_recv.at[2 * g + 1],
                sp_peer[1], tp,
            )
        )

    score(0)
    k_copies[1].wait_recv()
    score(1)

    before_id = lax.broadcasted_iota(jnp.int32, (rows, rows), 0)
    after_id = lax.broadcasted_iota(jnp.int32, (rows, rows), 1)
    expert_id = lax.broadcasted_iota(jnp.int32, (n_sp, rows), 0)
    hot = [(routes_t[k : k + 1, :] == expert_id).astype(F32) for k in range(TOPK)]
    before = dot(sum(hot).astype(BF16), as_bf16(before_id < after_id))
    ranks = [jnp.sum(before * h, axis=0, keepdims=True).astype(jnp.int32) for h in hot]
    slot_id = lax.broadcasted_iota(jnp.int32, (cap, rows), 0)
    slots_r = [jnp.zeros((1, rows), jnp.int32) for _ in range(TOPK)]
    for i in range(n_sp):
        here = [routes_t[k : k + 1, :] == sp_peer[i] for k in range(TOPK)]
        ids = [jnp.where(here[k], ranks[k], -1) for k in range(TOPK)]
        spare = jnp.where(
            (slot_id >= base + i * tail) & (slot_id < base + (i + 1) * tail), slot_id - i * tail, -2
        )
        rank_id = jnp.where(slot_id < base, slot_id, spare)
        pick_st[i * cap : (i + 1) * cap, :] = as_bf16((rank_id == ids[0]) | (rank_id == ids[1]))
        spot = [
            jnp.where(r < base, r + i * base, r - base + full + i * (extra + tail)) for r in ranks
        ]
        slots_r = [jnp.where(here[k], spot[k], slots_r[k]) for k in range(TOPK)]
    packed = jnp.concatenate(
        [s.astype(F32) for s in slots_r] + [mix_t[...], jnp.zeros((8 - 2 * TOPK, rows), F32)],
        axis=0,
    )
    packed = jnp.transpose(packed)
    slots_c = [packed[:, k : k + 1].astype(jnp.int32) for k in range(TOPK)]
    mix_c = [packed[:, TOPK + k : TOPK + k + 1] for k in range(TOPK)]
    slot_lane = lax.broadcasted_iota(jnp.int32, mixers.shape[2:], 1)
    for g in range(groups):
        for k in range(TOPK):
            mixers[g, k] = as_bf16(slot_lane == slots_c[k] - g * pair)

    for g in range(1, groups):
        pass_kv(g)
        score(2 * g)
        if g > 1:
            k_copies[2 * g - 1].wait_recv()
            score(2 * g - 1)
    for q in (1, 2, 3):
        o_copies[q].wait_recv()
        part = wo.at[q, mine, :]
        o_copies[q, "pair"] = start(
            remote(part, part, v_send.at[q], v_recv.at[q], sp_peer[1], tp)
        )
    k_copies[n_sp - 1].wait_recv()
    score(n_sp - 1)

    p_copies = {}
    for c in range(chunks):

        def head_probs(h, carry):
            span = pl.ds(pl.multiple_of(c * stacked + h * chunk, 16), chunk)
            dest = pl.ds(pl.multiple_of(h * chunk, 16), chunk)
            peak = jnp.max(top[span, :], axis=1, keepdims=True)
            total = jnp.zeros((chunk, 128), F32)
            for lane in range(0, n_sp * rows, 256):
                p = jnp.exp(scores_st[span, lane : lane + 256] - peak)
                probs[dest, lane : lane + 256] = p.astype(BF16)
                total = total + p[:, 0:128] + p[:, 128:256]
            total = jnp.sum(total, axis=1, keepdims=True)
            denom[dest, :] = jnp.broadcast_to(total, (chunk, 128))
            return carry

        lax.fori_loop(0, heads, head_probs, 0)
        values_all = kv[...].reshape(n_sp * rows, 2 * E)
        weighted = dot(probs[...], values_all)[:, E:] / denom[:, 0:E]
        weighted = weighted.astype(BF16)
        att[0, c] = jnp.concatenate(
            [weighted[h * chunk : (h + 1) * chunk, :] for h in range(heads)], axis=1
        )
        for q in (3, 1, 2):
            p_copies[q, c] = start(
                remote(
                    att.at[0, c], att.at[q, c], p_send.at[q, c], p_recv.at[q, c], me, tp_peer[q]
                )
            )

    own_cols.wait()
    for q in (1, 2, 3):
        o_copies[q, "pair"].wait_recv()
    for c in range(chunks):
        at = slice(c * chunk, (c + 1) * chunk)
        total = residual[at, :].astype(F32) + dot(att[0, c], wo[0]).astype(BF16).astype(F32)
        for q in (1, 2, 3):
            p_copies[q, c].wait_recv()
            total = total + dot(att[q, c], wo[q]).astype(BF16).astype(F32)
        after[at, :] = total
    total = after[...]
    square_sum = jnp.sum(total * total, axis=1, keepdims=True)
    n_out[...] = jnp.transpose(jnp.broadcast_to(square_sum, (rows, 128)))[0:8, :]
    n_copies = {}
    for q in (3, 1, 2):
        n_copies[q] = start(
            remote(n_out, n_in.at[q], n_send.at[q], n_recv.at[q], me, tp_peer[q])
        )
    scaled = (total * gain[...]).astype(BF16)

    x_copies, a_copies, r_copies, s_copies = {}, {}, {}, {}
    y_copies, e_copies, z_copies = {}, {}, {}

    def spread(i):
        if i == n_sp:
            gathered = x_tail[0].astype(F32)
            for j in range(1, n_sp):
                x_copies[j, "tail"].wait_recv()
                gathered = gathered + x_tail[j].astype(F32)
            x_all[block(i), feats(0)] = gathered.astype(BF16)
        elif i:
            x_copies[i].wait_recv()
        part = x_all.at[block(i), feats(0)]
        for q in (1, 2):
            a_copies[q, i] = start(
                remote(part, part, a_send.at[q, i], a_recv.at[q, i], me, tp_peer[q])
            )

    def relay(i):
        for q in (1, 2):
            whole = x_all.at[block(i), feats(q)]
            remote(whole, whole, a_send.at[q, i], a_recv.at[q, i], me, tp_peer[q]).wait_recv()
            part = x_all.at[block(i), feats(q, half, (q - 1) * half)]
            r_copies[q, i] = start(
                remote(part, part, r_send.at[q, i], r_recv.at[q, i], me, tp_peer[3 - q])
            )

    def await_block(i):
        for q in (1, 2):
            part = x_all.at[block(i), feats(3, half, (q - 1) * half)]
            remote(part, part, r_send.at[q, i], r_recv.at[q, i], me, tp_peer[3 - q]).wait_recv()

    def send_picked(i):
        picked = dot(pick_st[i * cap : (i + 1) * cap, :], scaled).astype(BF16)
        if i:
            x_out[i] = picked
            x_copies[i] = start(
                remote(
                    x_out.at[i, 0:base, :], x_all.at[block(i), feats(0)], x_send.at[i],
                    x_recv.at[i], sp_peer[i], tp,
                )
            )
            x_copies[i, "tail"] = start(
                remote(
                    x_out.at[i, base:cap, :], x_tail.at[i], g_send.at[i], g_recv.at[i],
                    sp_peer[i], tp,
                )
            )
        else:
            x_all[block(0), feats(0)] = picked[0:base]
            x_tail[0] = picked[base:cap]

    def send_scales(_):
        sum_rows = n_out[...]
        for q in (1, 2, 3):
            n_copies[q].wait_recv()
            sum_rows = sum_rows + n_in[q]
        scale_c = jnp.transpose(lax.rsqrt(sum_rows / features + norm_eps))[:, 0:1]
        lane = lax.broadcasted_iota(jnp.int32, (rows, 128), 1)
        for i in range(n_sp):
            spot = jnp.where(lane < base, lane + i * base, lane - base + full + i * extra)
            here = (spot == slots_c[0]) | (spot == slots_c[1])
            row = jnp.sum(jnp.where(here, scale_c, 0.0), axis=0, keepdims=True)
            tile = jnp.broadcast_to(row, (8, 128))
            if i:
                s_out[i] = tile
                s_copies[i] = start(
                    remote(s_out.at[i], s_in.at[i], s_send.at[i], s_recv.at[i], sp_peer[i], tp)
                )
            else:
                s_in[0] = tile

    tile = min(256, hidden)
    scaled_by = {0}

    def scales_of(i):
        if i not in scaled_by:
            s_copies[i].wait_recv()
            scaled_by.add(i)
        return s_in[i]

    def compute(g):
        members = [2 * g, 2 * g + 1]
        scale = [jnp.transpose(scales_of(i))[0:base, 0:1] for i in members]
        size = pair
        if g == groups - 1:
            tails = sum(scales_of(i) for i in range(n_sp))
            scale.append(jnp.transpose(tails)[base:cap, 0:1])
            members.append(n_sp)
            size = pair + extra
        scale = jnp.concatenate(scale, axis=0)
        for i in members:
            await_block(i)
        span = pl.ds(g * pair, size)
        used = pl.ds(0, size)

        def hidden_tile(t, carry):
            at = pl.ds(pl.multiple_of(t * tile, 128), tile)
            gate = dot(x_all[span, :], wg[:, at]) * scale
            up = dot(x_all[span, :], wu[:, at]) * scale
            act[used, at] = (gate / (1.0 + jnp.exp(-gate)) * up).astype(BF16)
            return carry

        lax.fori_loop(0, hidden // tile, hidden_tile, 0)
        diag = dot(act[used, :], wd[:, feats(3)]).astype(BF16)
        y_out[0, 0, span, :] = diag[:, :half]
        y_out[1, 0, span, :] = diag[:, half:]
        by_x = dot(act[used, :], wd[:, feats(1)]).astype(BF16)
        y_out[0, 1, span, :] = by_x[:, :half]
        y_keep[1, span, :] = by_x[:, half:]
        by_y = dot(act[used, :], wd[:, feats(2)]).astype(BF16)
        y_out[1, 1, span, :] = by_y[:, half:]
        y_keep[0, span, :] = by_y[:, :half]
        y_own[span, :] = dot(act[used, :], wd[:, feats(0)]).astype(BF16)

    def send_parts(i):
        for h in range(2):
            at = (h, slice(None), block(i), slice(None))
            y_copies[h, i] = start(
                remote(
                    y_out.at[at], y_in.at[at], y_send.at[h, i], y_recv.at[h, i], me, tp_peer[1 + h]
                )
            )

    def pass_on(i):
        for h in range(2):
            y_copies[h, i].wait_recv()
            both = y_in[h, 0, block(i), :].astype(F32) + y_keep[h, block(i), :].astype(F32)
            y_fwd[h, block(i), :] = both.astype(BF16)
            at = (h, block(i), slice(None))
            e_copies[h, i] = start(
                remote(
                    y_fwd.at[at], y_last.at[at], e_send.at[h, i], e_recv.at[h, i], me, tp_peer[2 - h]
                )
            )

    def finish(i):
        for h in range(2):
            e_copies[h, i].wait_recv()
            at = slice(h * half, (h + 1) * half)
            piece = y_own[block(i), at].astype(F32) + y_in[h, 1, block(i), :].astype(F32)
            piece = (piece + y_last[h, block(i), :].astype(F32)).astype(BF16)
            if i == n_sp:
                z_tail[:, at] = piece
                z_in[full : full + extra, at] = piece
            elif i:
                z_out[i, :, at] = piece
            else:
                z_in[0:base, at] = piece
        if i == n_sp:
            for j in range(1, n_sp):
                z_copies[j, "tail"] = start(
                    remote(
                        z_tail, z_in.at[pl.ds(full + j * extra, extra), :], h_send.at[j],
                        h_recv.at[j], sp_peer[j], tp,
                    )
                )
        elif i:
            z_copies[i] = start(
                remote(
                    z_out.at[i], z_in.at[block(i), :], z_send.at[i], z_recv.at[i], sp_peer[i], tp
                )
            )

    def mixed(g):
        for i in (2 * g, 2 * g + 1):
            if i:
                z_copies[i].wait_recv()
        size = pair
        if g == groups - 1:
            for j in range(1, n_sp):
                z_copies[j, "tail"].wait_recv()
            size = pair + n_sp * extra
        total = after[...]
        for k in range(TOPK):
            gathered = dot(mixers[g, k, :, 0:size], z_in[g * pair : g * pair + size, :])
            total = total + gathered * mix_c[k]
        return total

    def mix(g):
        after[...] = mixed(g)

    def mix_last(_):
        out[...] = mixed(0)

    def await_weights(_):
        for load in loads:
            load.wait()

    steps = {
        "X": send_picked, "S": spread, "R": relay, "N": send_scales, "W": await_weights,
        "C": compute, "Y": send_parts, "P": pass_on, "F": finish, "M": mix, "E": mix_last,
    }
    for step in order:
        steps[step[0]](int(step[1:] or 0))

    for copy in sent:
        copy.wait_send()


def turn_table(tokens):
    quarter = E // 4
    frequency = (rope_base ** (-np.arange(quarter) / quarter)).astype(np.float32)
    grid_rows = tokens // GRID_W

    def lanes_of(count, first):
        angles = np.arange(count, dtype=np.float32)[:, None] * frequency[None, :]
        blank = np.zeros((count, 2 * quarter), np.float32)
        cosine = np.concatenate([np.cos(angles)] * 2, axis=1)
        sines = np.concatenate([-np.sin(angles), np.sin(angles)], axis=1)
        both = []
        for part in (cosine, sines):
            head = [part, blank] if first else [blank, part]
            both += head * 2
        return np.concatenate(both, axis=1)

    return np.concatenate([lanes_of(grid_rows, True), lanes_of(GRID_W, False)], axis=0)


ORDER = (
    "X4", "X2", "X0", "X1", "S0", "S1", "R0", "X5", "S2", "X3", "S4", "X6", "R1", "S5", "N", "W",
    "S3", "R4", "X7", "R5", "S6", "R2", "C0", "S7", "R3", "S8", "C2", "Y5", "Y4", "R7", "R6",
    "R8", "C1", "Y2", "P5", "Y3", "P4", "C3", "F5", "P2", "Y7", "Y8", "Y6", "F2", "F4", "P3",
    "P7", "P8", "P6", "Y1", "Y0", "F7", "F8", "F3", "M2", "P1", "F6", "P0", "F1", "M1", "M3",
    "F0", "E",
)


def fused_shards(
    n_sp,
    n_tp,
    query_heads,
    key_heads,
    value_heads,
    q_gain,
    k_gain,
    out_weight,
    residual,
    norm_gain,
    routes,
    route_weights,
    w_gate,
    w_up,
    w_down,
):
    rows, cols = residual.shape
    width = query_heads.shape[1]
    heads = width // E
    hidden = w_gate.shape[2]
    features = cols * n_tp
    cap = 5 * rows * TOPK // (4 * n_sp) + 1
    tail = cap % ROW_TILE or ROW_TILE
    base = cap - tail
    extra = -(-n_sp * tail // ROW_TILE) * ROW_TILE
    cap = base + extra
    slots = n_sp * base + extra
    pair = 2 * base
    half = cols // 2
    chunks = 4
    chunk = rows // chunks
    dma = pltpu.SemaphoreType.DMA
    vmem = pl.BlockSpec(memory_space=VMEM)
    hbm = pl.BlockSpec(memory_space=pl.ANY)
    table = jnp.asarray(turn_table(n_sp * rows))
    small = (
        query_heads, key_heads, value_heads, q_gain.reshape(1, E), k_gain.reshape(1, E), table,
        residual, norm_gain.reshape(1, cols), routes.T, route_weights.T,
    )
    total = pl.pallas_call(
        functools.partial(fused_kernel, n_sp, n_tp, base, tail, chunks, ORDER),
        out_shape=jax.ShapeDtypeStruct((rows, cols), F32),
        in_specs=[hbm] * (4 + len(small)),
        out_specs=vmem,
        scratch_shapes=[VMEM(array.shape, array.dtype) for array in small] + [
            VMEM((features, hidden), BF16),
            VMEM((features, hidden), BF16),
            VMEM((hidden, features), BF16),
            VMEM((n_tp, width, cols), BF16),
            VMEM((rows, 2 * E), BF16),
            VMEM((n_sp, rows, 2 * E), BF16),
            VMEM((heads * rows, 2 * E), BF16),
            VMEM((heads * rows, n_sp * rows), F32),
            VMEM((heads * rows, 128), F32),
            VMEM((heads * chunk, n_sp * rows), BF16),
            VMEM((heads * chunk, 128), F32),
            VMEM((n_tp, chunks, chunk, width), BF16),
            VMEM((n_sp * cap, rows), BF16),
            VMEM((n_sp // 2, TOPK, rows, pair + n_sp * extra), BF16),
            VMEM((rows, cols), F32),
            VMEM((8, rows), F32),
            VMEM((n_tp, 8, rows), F32),
            VMEM((n_sp, 8, 128), F32),
            VMEM((n_sp, 8, 128), F32),
            VMEM((n_sp, cap, cols), BF16),
            VMEM((n_sp, extra, cols), BF16),
            VMEM((slots, features), BF16),
            VMEM((pair + extra, hidden), BF16),
            VMEM((2, 2, slots, half), BF16),
            VMEM((2, 2, slots, half), BF16),
            VMEM((slots, cols), BF16),
            VMEM((2, slots, half), BF16),
            VMEM((2, slots, half), BF16),
            VMEM((2, slots, half), BF16),
            VMEM((n_sp, base, cols), BF16),
            VMEM((extra, cols), BF16),
            VMEM((n_sp * cap, cols), BF16),
            dma((len(small),)),
            dma((4,)),
            dma((n_tp,)), dma((n_tp,)),
            dma((n_tp,)), dma((n_tp,)),
            dma((n_sp,)), dma((n_sp,)),
            dma((n_tp, chunks)), dma((n_tp, chunks)),
            dma((n_tp,)), dma((n_tp,)),
            dma((n_sp,)), dma((n_sp,)),
            dma((n_sp,)), dma((n_sp,)),
            dma((n_sp,)), dma((n_sp,)),
            dma((3, n_sp + 1)), dma((3, n_sp + 1)),
            dma((3, n_sp + 1)), dma((3, n_sp + 1)),
            dma((2, n_sp + 1)), dma((2, n_sp + 1)),
            dma((2, n_sp + 1)), dma((2, n_sp + 1)),
            dma((n_sp,)), dma((n_sp,)),
            dma((n_sp,)), dma((n_sp,)),
        ],
        compiler_params=pltpu.CompilerParams(
            collective_id=2, has_side_effects=True, vmem_limit_bytes=60 * 1024 * 1024
        ),
    )(out_weight, w_gate[0], w_up[0], w_down[0], *small)
    return total.astype(BF16)


def solution(mesh):
    n_sp, n_tp = mesh.shape["sp"], mesh.shape["tp"]
    local = fused_shards if n_tp == 4 and n_sp == 8 else shards
    return jax.shard_map(
        functools.partial(local, n_sp, n_tp),
        mesh=mesh,
        in_specs=(
            P("sp", "tp"),
            P("sp", None),
            P("sp", None),
            P(),
            P(),
            P("tp", None),
            P("sp", "tp"),
            P("tp"),
            P("sp", None),
            P("sp", None),
            P("sp", None, "tp"),
            P("sp", None, "tp"),
            P("sp", "tp", None),
        ),
        out_specs=P("sp", "tp"),
        check_vma=False,
    )
```

```python
import functools

import jax
import jax.numpy as jnp
import numpy as np
from jax import lax
from jax.experimental import pallas as pl
from jax.experimental.pallas import tpu as pltpu
from jax.sharding import PartitionSpec as P

D = 2048
HQ = 16
KV = 4
E = 64
TOPK = 2
GRID_W = 64

norm_eps = 1e-06
rope_base = 10000.0

MESH = pl.DeviceIdType.MESH
VMEM = pltpu.VMEM
F32 = jnp.float32
BF16 = jnp.bfloat16
ROW_TILE = 8


def normalize(values_f, gain):
    mean_sq = jnp.mean(values_f * values_f, axis=-1, keepdims=True)
    return values_f * lax.rsqrt(mean_sq + norm_eps) * gain


def rotate(values_f, positions):
    head_width = values_f.shape[-1]
    half_width = head_width // 2
    quarter_width = half_width // 2
    frequency = rope_base ** (-jnp.arange(quarter_width, dtype=jnp.float32) / quarter_width)
    grid_rows = (positions // GRID_W).astype(jnp.float32)
    grid_cols = (positions % GRID_W).astype(jnp.float32)
    shape = (values_f.shape[0],) + (1,) * (values_f.ndim - 2) + (quarter_width,)
    pieces = []
    for coords, offset_lo in ((grid_rows, 0), (grid_cols, half_width)):
        angles = coords[:, None] * frequency[None, :]
        cosine = jnp.cos(angles).reshape(shape)
        sines = jnp.sin(angles).reshape(shape)
        first_part = values_f[..., offset_lo : offset_lo + quarter_width]
        second_part = values_f[..., offset_lo + quarter_width : offset_lo + half_width]
        pieces.append(first_part * cosine - second_part * sines)
        pieces.append(second_part * cosine + first_part * sines)
    return jnp.concatenate(pieces, axis=-1)


def dot(a, b):
    return jnp.dot(a, b, preferred_element_type=F32)


def tp_offset(tp, n_tp, q):
    if n_tp == 4:
        x = lax.rem(lax.rem(tp, 2) + q % 2, 2)
        y = lax.rem(lax.div(tp, 2) + q // 2, 2)
        return y * 2 + x
    return lax.rem(tp + q, n_tp)


def tp_origin(tp, n_tp, q):
    return tp_offset(tp, n_tp, q if n_tp == 4 else n_tp - q)


def remote(src, dst, send_sem, recv_sem, sp, tp):
    return pltpu.make_async_remote_copy(
        src_ref=src, dst_ref=dst, send_sem=send_sem, recv_sem=recv_sem,
        device_id=(sp, tp), device_id_type=MESH,
    )


def gather_kernel(
    n_sp, n_tp, own, weight, out, weight_out, send, recv, send2, recv2, w_send, w_recv,
    v_send, v_recv
):
    me = lax.axis_index("sp")
    tp = lax.axis_index("tp")
    chips = n_sp // 2
    core = lax.rem(me, 2)
    z = lax.div(me, 2)
    partner = z * 2 + 1 - core
    barrier = pltpu.get_barrier_semaphore()
    pl.semaphore_signal(barrier, inc=1, device_id=(partner, tp), device_id_type=MESH)
    for j in range(1, chips):
        pl.semaphore_signal(
            barrier, inc=1, device_id=(lax.rem(z + j, chips) * 2 + core, tp), device_id_type=MESH
        )
    for q in range(1, n_tp):
        pl.semaphore_signal(
            barrier, inc=1, device_id=(me, tp_offset(tp, n_tp, q)), device_id_type=MESH
        )
    pl.semaphore_wait(barrier, chips + n_tp - 1)
    first = []
    for j in range(1, chips):
        copy = remote(own, out.at[me], send.at[j], recv.at[j], lax.rem(z + j, chips) * 2 + core, tp)
        copy.start()
        first.append(copy)
    swap = remote(own, out.at[me], send2.at[0], recv2.at[0], partner, tp)
    swap.start()
    out[me] = own[...]
    cols = weight_out.shape[2]
    depth = weight.shape[0] // 2
    mine = pl.ds(pl.multiple_of(core * depth, 16), depth)
    third = {}
    for q in range(n_tp - 1, 0, -1):
        peer = tp_offset(tp, n_tp, q)
        part = weight.at[mine, pl.ds(pl.multiple_of(peer * cols, 128), cols)]
        third[q] = remote(
            part, weight_out.at[tp, mine, :], w_send.at[q], w_recv.at[q], me, peer
        )
        third[q].start()
    weight_out[tp] = weight[:, pl.ds(pl.multiple_of(tp * cols, 128), cols)]
    second = [swap]
    for j in range(1, chips):
        first[j - 1].wait_recv()
        source = lax.rem(z + chips - j, chips) * 2 + core
        copy = remote(out.at[source], out.at[source], send2.at[j], recv2.at[j], partner, tp)
        copy.start()
        second.append(copy)
    for q in range(1, n_tp):
        third[q].wait_recv()
        part = weight_out.at[tp_origin(tp, n_tp, q), mine, :]
        copy = remote(part, part, v_send.at[q], v_recv.at[q], partner, tp)
        copy.start()
        second.append(copy)
    for copy in second:
        copy.wait()
    for copy in first + list(third.values()):
        copy.wait_send()


def gather_kv(n_sp, n_tp, own, weight):
    rows, width = own.shape
    depth, feats = weight.shape
    return pl.pallas_call(
        functools.partial(gather_kernel, n_sp, n_tp),
        out_shape=(
            jax.ShapeDtypeStruct((n_sp, rows, width), own.dtype),
            jax.ShapeDtypeStruct((n_tp, depth, feats // n_tp), weight.dtype),
        ),
        in_specs=[pl.BlockSpec(memory_space=VMEM)] * 2,
        out_specs=[pl.BlockSpec(memory_space=VMEM)] * 2,
        scratch_shapes=[pltpu.SemaphoreType.DMA((n_sp // 2,))] * 4
        + [pltpu.SemaphoreType.DMA((n_tp,))] * 4,
        compiler_params=pltpu.CompilerParams(collective_id=0, has_side_effects=True),
    )(own, weight)


def layer_kernel(
    n_sp, n_tp, capacity, groups,
    attended, out_weight, residual, gain, routes, routes_t, mix_w, w_gate, w_up, w_down,
    out,
    wg, wu, wd, p_in, after, n_out, n_in, x_out, x_all, act, y_out, y_in, y_own, y_keep, y_fwd, y_last,
    z_out, z_in,
    w_sem, p_send, p_recv, n_send, n_recv, x_send, x_recv, a_send, a_recv, r_send, r_recv,
    y_send, y_recv, e_send, e_recv, z_send, z_recv,
):
    me = lax.axis_index("sp")
    tp = lax.axis_index("tp")
    rows, cols = residual.shape
    hidden = w_gate.shape[1]
    square = n_tp == 4

    def to_tp(q):
        return tp_offset(tp, n_tp, q)

    def from_tp(q):
        return tp_origin(tp, n_tp, q)

    def to_sp(j):
        return lax.rem(me + j, n_sp)

    def from_sp(j):
        return lax.rem(me + n_sp - j, n_sp)

    def feats(t, width=cols, shift=0):
        return pl.ds(pl.multiple_of(t * cols + shift, 128), width)

    def block(j):
        return pl.ds(j * capacity, capacity)

    loads = [
        pltpu.make_async_copy(s, d, w_sem.at[i])
        for i, (s, d) in enumerate(((w_gate, wg), (w_up, wu), (w_down, wd)))
    ]
    for load in loads:
        load.start()

    barrier = pltpu.get_barrier_semaphore()
    for q in range(1, n_tp):
        pl.semaphore_signal(barrier, inc=1, device_id=(me, to_tp(q)), device_id_type=MESH)
    for j in range(1, n_sp):
        pl.semaphore_signal(barrier, inc=1, device_id=(to_sp(j), tp), device_id_type=MESH)
    pl.semaphore_wait(barrier, n_tp - 1 + n_sp - 1)

    order = [3, 1, 2] if square else list(range(1, n_tp))
    p_copies = {}
    for q in order:
        p_copies[q] = remote(attended, p_in.at[q], p_send.at[q], p_recv.at[q], me, to_tp(q))
        p_copies[q].start()
    total = dot(attended[...], out_weight[tp]).astype(BF16).astype(F32)

    tri = lax.broadcasted_iota(jnp.int32, (rows, rows), 0)
    tri_c = lax.broadcasted_iota(jnp.int32, (rows, rows), 1)
    upper = (tri < tri_c).astype(F32).astype(BF16)
    lower = (tri > tri_c).astype(F32).astype(BF16)
    expert_rows = lax.broadcasted_iota(jnp.int32, (n_sp, rows), 0)
    expert_cols = lax.broadcasted_iota(jnp.int32, (rows, n_sp), 1)
    hot_r = [(routes_t[k : k + 1, :] == expert_rows).astype(F32) for k in range(TOPK)]
    hot_c = [(routes[:, k : k + 1] == expert_cols).astype(F32) for k in range(TOPK)]
    before_r = dot(sum(hot_r).astype(BF16), upper)
    before_c = dot(lower, sum(hot_c).astype(BF16))
    slot_r, slot_c = [], []
    for k in range(TOPK):
        rank = jnp.sum(before_r * hot_r[k], axis=0, keepdims=True).astype(jnp.int32)
        rel = routes_t[k : k + 1, :] - me
        rel = jnp.where(rel < 0, rel + n_sp, rel)
        slot_r.append(rel * capacity + rank)
        rank = jnp.sum(before_c * hot_c[k], axis=1, keepdims=True).astype(jnp.int32)
        rel = routes[:, k : k + 1] - me
        rel = jnp.where(rel < 0, rel + n_sp, rel)
        slot_c.append(rel * capacity + rank)

    total = residual[...].astype(F32) + total
    for q in [1, 2, 3] if square else order:
        p_copies[q].wait_recv()
        total = total + dot(p_in[q], out_weight[from_tp(q)]).astype(BF16).astype(F32)
    after[...] = total
    square_sum = jnp.sum(total * total, axis=1, keepdims=True)
    as_rows = jnp.transpose(jnp.broadcast_to(square_sum, (rows, 128)))
    n_out[...] = as_rows[0:8, :]
    n_copies = []
    for q in range(1, n_tp):
        copy = remote(n_out, n_in.at[q], n_send.at[q], n_recv.at[q], me, to_tp(q))
        copy.start()
        n_copies.append(copy)
    sum_rows = n_out[...]
    for q in range(1, n_tp):
        n_copies[q - 1].wait_recv()
        sum_rows = sum_rows + n_in[q]
    all_sum = jnp.transpose(jnp.broadcast_to(sum_rows[0:1, :], (128, rows)))[:, 0:1]
    normed = (after[...] * lax.rsqrt(all_sum / D + norm_eps) * gain[...]).astype(BF16)

    x_copies = {}
    slot_id = lax.broadcasted_iota(jnp.int32, (capacity, rows), 0)
    for j in list(range(1, n_sp)) + [0]:
        ids = slot_id + j * capacity
        pick = ((ids == slot_r[0]) | (ids == slot_r[1])).astype(F32).astype(BF16)
        picked = dot(pick, normed).astype(BF16)
        x_out[j] = picked
        if j:
            x_copies[j] = remote(
                x_out.at[j], x_all.at[block(j), feats(tp)], x_send.at[j], x_recv.at[j], to_sp(j), tp
            )
            x_copies[j].start()
        else:
            x_all[block(0), feats(tp)] = picked

    direct = [1, 2] if square else list(range(1, n_tp))
    a_copies, r_copies = {}, {}

    def spread(j):
        if j:
            x_copies[j].wait_recv()
        part = x_all.at[block(j), feats(tp)]
        for q in direct:
            a_copies[q, j] = remote(part, part, a_send.at[q, j], a_recv.at[q, j], me, to_tp(q))
            a_copies[q, j].start()

    def await_direct(q, j):
        part = x_all.at[block(j), feats(from_tp(q))]
        remote(part, part, a_send.at[q, j], a_recv.at[q, j], me, to_tp(q)).wait_recv()

    def relay(j):
        half = cols // 2
        for i, q in enumerate((1, 2)):
            await_direct(q, j)
            part = x_all.at[block(j), feats(to_tp(q), half, i * half)]
            r_copies[i, j] = remote(part, part, r_send.at[i, j], r_recv.at[i, j], me, to_tp(3 - q))
            r_copies[i, j].start()

    def await_block(j):
        if square:
            half = cols // 2
            for i in range(2):
                part = x_all.at[block(j), feats(to_tp(3), half, i * half)]
                remote(part, part, r_send.at[i, j], r_recv.at[i, j], me, tp_peer).wait_recv()
        else:
            for q in direct:
                await_direct(q, j)

    tp_peer = to_tp(1)
    lag = 2
    for j in range(n_sp + lag):
        if j < n_sp:
            spread(j)
        if square and j >= lag:
            relay(j - lag)

    for load in loads:
        load.wait()
    per = n_sp // groups
    m = per * capacity
    tile = min(256, hidden)
    y_copies, e_copies, z_copies = {}, {}, {}
    half = cols // 2

    def send_parts(j):
        for i in range(2):
            at = (i, slice(None), block(j), slice(None))
            y_copies[i, j] = remote(
                y_out.at[at], y_in.at[at], y_send.at[i, j], y_recv.at[i, j], me, to_tp(1 + i)
            )
            y_copies[i, j].start()

    def pass_on(j):
        for i in range(2):
            y_copies[i, j].wait_recv()
            both = y_in[i, 0, block(j), :].astype(F32) + y_keep[i, block(j), :].astype(F32)
            y_fwd[i, block(j), :] = both.astype(BF16)
            at = (i, block(j), slice(None))
            e_copies[i, j] = remote(
                y_fwd.at[at], y_last.at[at], e_send.at[i, j], e_recv.at[i, j], me, to_tp(2 - i)
            )
            e_copies[i, j].start()

    def finish(j):
        if square:
            pieces = []
            for i in range(2):
                e_copies[i, j].wait_recv()
                piece = y_own[block(j), i * half : (i + 1) * half].astype(F32)
                piece = piece + y_in[i, 1, block(j), :].astype(F32)
                pieces.append((piece + y_last[i, block(j), :].astype(F32)).astype(BF16))
        else:
            acc = y_own[block(j), :].astype(F32)
            for q in range(1, n_tp):
                y_copies[q, j].wait_recv()
                acc = acc + y_in[q, block(j), :].astype(F32)
            pieces = [acc.astype(BF16)]
        width = cols // len(pieces)
        for i, piece in enumerate(pieces):
            at = slice(i * width, (i + 1) * width)
            if j == 0:
                z_in[0:capacity, at] = piece
            else:
                z_out[j, :, at] = piece
        if j:
            z_copies[j] = remote(
                z_out.at[j], z_in.at[block(j), :], z_send.at[j], z_recv.at[j], from_sp(j), tp
            )
            z_copies[j].start()

    for g in range(groups):
        for b in range(per):
            await_block(g * per + b)
        span = pl.ds(g * m, m)

        def hidden_tile(i, carry):
            at = pl.ds(pl.multiple_of(i * tile, 128), tile)
            gate = dot(x_all[span, :], wg[:, at])
            up = dot(x_all[span, :], wu[:, at])
            act[:, at] = (gate / (1.0 + jnp.exp(-gate)) * up).astype(BF16)
            return carry

        lax.fori_loop(0, hidden // tile, hidden_tile, 0)
        blocks = range(g * per, (g + 1) * per)
        if square:
            diag = dot(act[...], wd[:, feats(to_tp(3))]).astype(BF16)
            y_out[0, 0, span, :] = diag[:, :half]
            y_out[1, 0, span, :] = diag[:, half:]
            by_x = dot(act[...], wd[:, feats(to_tp(1))]).astype(BF16)
            y_out[0, 1, span, :] = by_x[:, :half]
            y_keep[1, span, :] = by_x[:, half:]
            by_y = dot(act[...], wd[:, feats(to_tp(2))]).astype(BF16)
            y_out[1, 1, span, :] = by_y[:, half:]
            y_keep[0, span, :] = by_y[:, :half]
            for j in blocks:
                send_parts(j)
        else:
            for q in order:
                y_out[q, span, :] = dot(act[...], wd[:, feats(to_tp(q))]).astype(BF16)
                for j in blocks:
                    at = (q, block(j), slice(None))
                    y_copies[q, j] = remote(
                        y_out.at[at], y_in.at[at], y_send.at[q, j], y_recv.at[q, j], me, to_tp(q)
                    )
                    y_copies[q, j].start()
        y_own[span, :] = dot(act[...], wd[:, feats(tp)]).astype(BF16)
    for j in range(n_sp + lag):
        if square and j < n_sp:
            pass_on(j)
        if j >= lag:
            finish(j - lag)

    slot_lane = lax.broadcasted_iota(jnp.int32, (rows, n_sp * capacity), 1)
    picks = [(slot_lane == slot_c[k]).astype(F32).astype(BF16) for k in range(TOPK)]
    for j in range(1, n_sp):
        z_copies[j].wait_recv()
    mix = dot(picks[0], z_in[...]) * mix_w[:, 0:1]
    mix = mix + dot(picks[1], z_in[...]) * mix_w[:, 1:2]
    out[...] = (after[...] + mix).astype(BF16)

    for copies in (p_copies, x_copies, a_copies, r_copies, y_copies, e_copies, z_copies):
        for copy in copies.values():
            copy.wait_send()
    for copy in n_copies:
        copy.wait_send()


def layer(
    n_sp, n_tp, attended, out_weight, residual, norm_gain, routes, route_weights,
    w_gate, w_up, w_down,
):
    rows, cols = residual.shape
    hidden = w_gate.shape[1]
    capacity = 5 * rows * TOPK // (4 * n_sp) + 1
    capacity = -(-capacity // ROW_TILE) * ROW_TILE
    groups = 2
    slots = n_sp * capacity
    square = n_tp == 4
    parts = (2, 2, slots, cols // 2) if square else (n_tp, slots, cols)
    relayed = (2, slots, cols // 2) if square else (2, 8, 128)
    dma = pltpu.SemaphoreType.DMA
    vmem = pl.BlockSpec(memory_space=VMEM)
    hbm = pl.BlockSpec(memory_space=pl.ANY)
    return pl.pallas_call(
        functools.partial(layer_kernel, n_sp, n_tp, capacity, groups),
        out_shape=jax.ShapeDtypeStruct((rows, cols), BF16),
        in_specs=[vmem] * 7 + [hbm] * 3,
        out_specs=vmem,
        scratch_shapes=[
            VMEM((D, hidden), BF16),
            VMEM((D, hidden), BF16),
            VMEM((hidden, D), BF16),
            VMEM((n_tp,) + attended.shape, BF16),
            VMEM((rows, cols), F32),
            VMEM((8, rows), F32),
            VMEM((n_tp, 8, rows), F32),
            VMEM((n_sp, capacity, cols), BF16),
            VMEM((slots, D), BF16),
            VMEM((slots // groups, hidden), BF16),
            VMEM(parts, BF16),
            VMEM(parts, BF16),
            VMEM((slots, cols), BF16),
            VMEM(relayed, BF16),
            VMEM(relayed, BF16),
            VMEM(relayed, BF16),
            VMEM((n_sp, capacity, cols), BF16),
            VMEM((slots, cols), BF16),
            dma((3,)),
            dma((n_tp,)), dma((n_tp,)),
            dma((n_tp,)), dma((n_tp,)),
            dma((n_sp,)), dma((n_sp,)),
            dma((n_tp, n_sp)), dma((n_tp, n_sp)),
            dma((2, n_sp)), dma((2, n_sp)),
            dma((n_tp, n_sp)), dma((n_tp, n_sp)),
            dma((2, n_sp)), dma((2, n_sp)),
            dma((n_sp,)), dma((n_sp,)),
        ],
        compiler_params=pltpu.CompilerParams(
            collective_id=1, has_side_effects=True, vmem_limit_bytes=60 * 1024 * 1024
        ),
    )(
        attended, out_weight, residual, norm_gain.reshape(1, cols), routes, routes.T,
        route_weights, w_gate, w_up, w_down,
    )


def shards(
    n_sp,
    n_tp,
    query_heads,
    key_heads,
    value_heads,
    q_gain,
    k_gain,
    out_weight,
    residual,
    norm_gain,
    routes,
    route_weights,
    w_gate,
    w_up,
    w_down,
):
    tok_rows = query_heads.shape[0]
    head_local = query_heads.shape[1] // E
    group_size = HQ // KV
    kv_count = max(head_local // group_size, 1)
    per_kv = head_local // kv_count
    tp_index = lax.axis_index("tp")
    sp_index = lax.axis_index("sp")
    kv_first = tp_index * head_local // group_size
    positions = sp_index * tok_rows + jnp.arange(tok_rows, dtype=jnp.int32)
    query_f = query_heads.astype(jnp.float32).reshape(tok_rows, kv_count, per_kv, E)
    q_turned = rotate(normalize(query_f, q_gain), positions).astype(jnp.bfloat16)
    key_cols = lax.dynamic_slice_in_dim(key_heads, kv_first * E, kv_count * E, 1)
    value_cols = lax.dynamic_slice_in_dim(value_heads, kv_first * E, kv_count * E, 1)
    key_f = key_cols.astype(jnp.float32).reshape(tok_rows, kv_count, E)
    k_turned = rotate(normalize(key_f, k_gain), positions).astype(jnp.bfloat16)
    width = kv_count * E
    own = jnp.concatenate([k_turned.reshape(tok_rows, width), value_cols], axis=1)
    both, out_weight = gather_kv(n_sp, n_tp, own, out_weight)
    both = both.reshape(n_sp * tok_rows, 2 * width)
    key_block = both[:, :width].reshape(-1, kv_count, E)
    value_block = both[:, width:].reshape(-1, kv_count, E)
    scores = jnp.einsum(
        "qcge,kce->cgqk", q_turned, key_block, preferred_element_type=jnp.float32
    ) * E ** (-0.5)
    new_max = jnp.max(scores, axis=-1)
    exped = jnp.exp(scores - new_max[..., None])
    denominator = jnp.sum(exped, axis=-1)
    weighted = jnp.einsum(
        "cgqk,kce->cgqe",
        exped.astype(jnp.bfloat16),
        value_block,
        preferred_element_type=jnp.float32,
    )
    attended = (weighted / denominator[..., None]).astype(jnp.bfloat16)
    attended = attended.transpose(2, 0, 1, 3).reshape(tok_rows, head_local * E)
    return layer(
        n_sp, n_tp, attended, out_weight, residual, norm_gain, routes, route_weights,
        w_gate[0], w_up[0], w_down[0],
    )


def flip(index, bits, size):
    mirrored = 0
    step = 1
    while step < size:
        digit = lax.rem(lax.div(index, step), 2)
        mirrored = mirrored + step * (1 - digit if bits & step else digit)
        step *= 2
    return mirrored


def swap_lanes(lanes, quarter):
    return jnp.where(jnp.bitwise_and(lanes, quarter) == 0, lanes + quarter, lanes - quarter)


def swap_quarters(gain, quarter):
    parts = [gain[:, i * quarter : (i + 1) * quarter] for i in (1, 0, 3, 2)]
    return jnp.concatenate(parts, axis=1)


def as_bf16(mask):
    return mask.astype(F32).astype(BF16)


def square_sums(values_f, same_head):
    squared = values_f * values_f
    high = squared.astype(BF16)
    low = (squared - high.astype(F32)).astype(BF16)
    return dot(high, same_head) + dot(low, same_head)


def fused_kernel(
    n_sp, n_tp, base, tail, chunks, order,
    weight, w_gate, w_up, w_down, *rest,
):
    small, out, staged, rest = rest[:10], rest[10], rest[11:21], rest[21:]
    query, keys, values, q_gain, k_gain, table, residual, gain, routes_t, mix_t = staged
    (
        wg, wu, wd, wo, own, kv, q_st, scores_st, top, probs, denom, att, pick_st, mixers,
        scaled, after, n_out, n_in, s_out, s_in, x_out, x_tail, x_all, act,
        y_out, y_in, y_own, y_keep, y_fwd, y_last, z_out, z_tail, z_in,
        l_sem, w_sem, o_send, o_recv, v_send, v_recv, k_send, k_recv, p_send, p_recv,
        n_send, n_recv, s_send, s_recv, x_send, x_recv, g_send, g_recv, a_send, a_recv, r_send, r_recv,
        y_send, y_recv, e_send, e_recv, z_send, z_recv, h_send, h_recv,
    ) = rest
    me = lax.axis_index("sp")
    tp = lax.axis_index("tp")
    rows, cols = out.shape
    hidden = wg.shape[1]
    features = cols * n_tp
    width = query.shape[1]
    heads = width // E
    chunk = rows // chunks
    stacked = heads * chunk
    groups = n_sp // 2
    pair = 2 * base
    extra = -(-n_sp * tail // 8) * 8
    cap = base + extra
    full = n_sp * base
    half = cols // 2
    core = lax.rem(me, 2)
    sp_peer = [flip(me, i, n_sp) for i in range(n_sp)]
    tp_peer = [flip(tp, q, n_tp) for q in range(n_tp)]
    sent = []

    def start(copy):
        copy.start()
        sent.append(copy)
        return copy

    def feats(q, size=cols, shift=0):
        return pl.ds(pl.multiple_of(tp_peer[q] * cols + shift, 128), size)

    def block(i):
        return pl.ds(i * base, base if i < n_sp else extra)

    barrier = pltpu.get_barrier_semaphore()
    for q in range(1, n_tp):
        pl.semaphore_signal(barrier, inc=1, device_id=(me, tp_peer[q]), device_id_type=MESH)
    for i in range(1, n_sp):
        pl.semaphore_signal(barrier, inc=1, device_id=(sp_peer[i], tp), device_id_type=MESH)
    fetches = [
        pltpu.make_async_copy(s, d, l_sem.at[i]) for i, (s, d) in enumerate(zip(small, staged))
    ]
    for i in (1, 2, 4, 5, 0, 3, 8, 9, 6, 7):
        fetches[i].start()
    own_cols = pltpu.make_async_copy(weight.at[:, feats(0)], wo.at[0], w_sem.at[3])
    own_cols.start()

    quarter = E // 4
    kv_first = lax.div(tp * heads * KV, HQ)
    source = lax.broadcasted_iota(jnp.int32, (keys.shape[1], 2 * E), 0) - kv_first * E
    lanes = lax.broadcasted_iota(jnp.int32, (keys.shape[1], 2 * E), 1)
    first = lanes < E
    for i in (1, 2, 4, 5):
        fetches[i].wait()
    k_f = dot(keys[...], as_bf16((source == lanes) & first))
    k_swap = dot(keys[...], as_bf16((source == swap_lanes(lanes, quarter)) & first))
    v_f = dot(values[...], as_bf16((source == lanes - E) & (lanes >= E)))
    grid_rows = rows // GRID_W
    all_rows = table.shape[0] - GRID_W
    by_col = table[all_rows:, :]
    turns = jnp.concatenate(
        [by_col + table[pl.ds(me * grid_rows + j, 1), :] for j in range(grid_rows)], axis=0
    )
    cosine, sine = turns[:, : 2 * E], turns[:, 2 * E :]
    gain_k = jnp.concatenate([k_gain[...]] * 2, axis=1)
    gain_ks = jnp.concatenate([swap_quarters(k_gain[...], quarter)] * 2, axis=1)
    sums = square_sums(k_f, jnp.ones((2 * E, 2 * E), BF16))
    k_turned = (k_f * gain_k) * cosine + (k_swap * gain_ks) * sine
    k_turned = k_turned * lax.rsqrt(sums / E + norm_eps)
    own[...] = (k_turned + v_f).astype(BF16)

    pl.semaphore_wait(barrier, n_tp - 1 + n_sp - 1)

    k_copies = {}
    for g in range(1, groups):
        k_copies[2 * g] = start(
            remote(own, kv.at[2 * g], k_send.at[2 * g], k_recv.at[2 * g], sp_peer[2 * g], tp)
        )
    k_copies[1] = start(remote(own, kv.at[1], k_send.at[1], k_recv.at[1], sp_peer[1], tp))
    depth = wo.shape[1] // 2
    mine = pl.ds(pl.multiple_of(core * depth, 16), depth)
    o_copies = {}
    for q in (3, 1, 2):
        o_copies[q] = start(
            remote(
                weight.at[mine, feats(q)], wo.at[q, mine, :], o_send.at[q], o_recv.at[q],
                me, tp_peer[q],
            )
        )
    loads = [
        pltpu.make_async_copy(s, d, w_sem.at[i])
        for i, (s, d) in enumerate(((w_gate, wg), (w_up, wu), (w_down, wd)))
    ]
    for load in loads:
        load.start()
    kv[0] = own[...]

    for i in (0, 3, 8, 9, 6, 7):
        fetches[i].wait()
    from_lane = lax.broadcasted_iota(jnp.int32, (width, width), 0)
    to_lane = lax.broadcasted_iota(jnp.int32, (width, width), 1)
    head_bits = width - E
    same = as_bf16(
        jnp.bitwise_and(from_lane, head_bits) == jnp.bitwise_and(to_lane, head_bits)
    )
    q_f = query[...].astype(F32)
    q_swap = dot(query[...], as_bf16(from_lane == swap_lanes(to_lane, quarter)))
    copies_of = width // (2 * E)
    gain_q = jnp.concatenate([q_gain[...]] * heads, axis=1)
    gain_qs = jnp.concatenate([swap_quarters(q_gain[...], quarter)] * heads, axis=1)
    q_turned = (q_f * gain_q) * jnp.concatenate([cosine] * copies_of, axis=1)
    q_turned = q_turned + (q_swap * gain_qs) * jnp.concatenate([sine] * copies_of, axis=1)
    q_turned = q_turned * lax.rsqrt(square_sums(q_f, same) / E + norm_eps)
    q_turned = (q_turned * E ** (-0.5)).astype(BF16)
    q_st[...] = jnp.zeros_like(q_st)
    for c in range(chunks):
        for h in range(heads):
            q_st[pl.ds((c * heads + h) * chunk, chunk), 0:E] = q_turned[
                c * chunk : (c + 1) * chunk, h * E : (h + 1) * E
            ]

    def score(i):
        at = pl.ds(i * rows, rows)

        def score_chunk(c, carry):
            span = pl.ds(pl.multiple_of(c * rows, 16), rows)
            s = lax.dot_general(
                q_st[span, :], kv[i], (((1,), (1,)), ((), ())), preferred_element_type=F32
            )
            scores_st[span, at] = s
            folded = s[:, 0:128]
            for lane in range(128, rows, 128):
                folded = jnp.maximum(folded, s[:, lane : lane + 128])
            top[span, :] = folded if i == 0 else jnp.maximum(top[span, :], folded)
            return carry

        lax.fori_loop(0, heads, score_chunk, 0)

    def pass_kv(g):
        k_copies[2 * g].wait_recv()
        k_copies[2 * g + 1] = start(
            remote(
                kv.at[2 * g], kv.at[2 * g + 1], k_send.at[2 * g + 1], k_recv.at[2 * g + 1],
                sp_peer[1], tp,
            )
        )

    score(0)
    k_copies[1].wait_recv()
    score(1)

    before_id = lax.broadcasted_iota(jnp.int32, (rows, rows), 0)
    after_id = lax.broadcasted_iota(jnp.int32, (rows, rows), 1)
    expert_id = lax.broadcasted_iota(jnp.int32, (n_sp, rows), 0)
    hot = [(routes_t[k : k + 1, :] == expert_id).astype(F32) for k in range(TOPK)]
    before = dot(sum(hot).astype(BF16), as_bf16(before_id < after_id))
    ranks = [jnp.sum(before * h, axis=0, keepdims=True).astype(jnp.int32) for h in hot]
    slot_id = lax.broadcasted_iota(jnp.int32, (cap, rows), 0)
    slots_r = [jnp.zeros((1, rows), jnp.int32) for _ in range(TOPK)]
    for i in range(n_sp):
        here = [routes_t[k : k + 1, :] == sp_peer[i] for k in range(TOPK)]
        ids = [jnp.where(here[k], ranks[k], -1) for k in range(TOPK)]
        spare = jnp.where(
            (slot_id >= base + i * tail) & (slot_id < base + (i + 1) * tail), slot_id - i * tail, -2
        )
        rank_id = jnp.where(slot_id < base, slot_id, spare)
        pick_st[i * cap : (i + 1) * cap, :] = as_bf16((rank_id == ids[0]) | (rank_id == ids[1]))
        spot = [
            jnp.where(r < base, r + i * base, r - base + full + i * (extra + tail)) for r in ranks
        ]
        slots_r = [jnp.where(here[k], spot[k], slots_r[k]) for k in range(TOPK)]
    packed = jnp.concatenate(
        [s.astype(F32) for s in slots_r] + [mix_t[...], jnp.zeros((8 - 2 * TOPK, rows), F32)],
        axis=0,
    )
    packed = jnp.transpose(packed)
    slots_c = [packed[:, k : k + 1].astype(jnp.int32) for k in range(TOPK)]
    mix_c = [packed[:, TOPK + k : TOPK + k + 1] for k in range(TOPK)]
    slot_lane = lax.broadcasted_iota(jnp.int32, mixers.shape[2:], 1)
    for g in range(groups):
        for k in range(TOPK):
            mixers[g, k] = as_bf16(slot_lane == slots_c[k] - g * pair)

    for g in range(1, groups):
        pass_kv(g)
        score(2 * g)
        if g > 1:
            k_copies[2 * g - 1].wait_recv()
            score(2 * g - 1)
    for q in (1, 2, 3):
        o_copies[q].wait_recv()
        part = wo.at[q, mine, :]
        o_copies[q, "pair"] = start(
            remote(part, part, v_send.at[q], v_recv.at[q], sp_peer[1], tp)
        )
    k_copies[n_sp - 1].wait_recv()
    score(n_sp - 1)

    peaks = jnp.max(top[...], axis=1, keepdims=True)
    top[...] = jnp.broadcast_to(peaks, top.shape)
    p_copies = {}
    for c in range(chunks):
        for h in range(heads):
            span = pl.ds(c * stacked + h * chunk, chunk)
            dest = pl.ds(h * chunk, chunk)
            peak = top[span, :]
            total = jnp.zeros((chunk, 128), F32)
            for lane in range(0, n_sp * rows, 128):
                p = jnp.exp(scores_st[span, lane : lane + 128] - peak)
                probs[dest, lane : lane + 128] = p.astype(BF16)
                total = total + p
            denom[dest, :] = total
        values_all = kv[...].reshape(n_sp * rows, 2 * E)
        weighted = dot(probs[...], values_all)[:, E:]
        weighted = weighted / jnp.sum(denom[...], axis=1, keepdims=True)
        weighted = weighted.astype(BF16)
        att[0, c] = jnp.concatenate(
            [weighted[h * chunk : (h + 1) * chunk, :] for h in range(heads)], axis=1
        )
        for q in (3, 1, 2):
            p_copies[q, c] = start(
                remote(
                    att.at[0, c], att.at[q, c], p_send.at[q, c], p_recv.at[q, c], me, tp_peer[q]
                )
            )

    own_cols.wait()
    for q in (1, 2, 3):
        o_copies[q, "pair"].wait_recv()
    for c in range(chunks):
        at = slice(c * chunk, (c + 1) * chunk)
        for q in (1, 2, 3):
            p_copies[q, c].wait_recv()
        total = residual[at, :].astype(F32)
        for q in range(n_tp):
            total = total + dot(att[q, c], wo[q]).astype(BF16).astype(F32)
        after[at, :] = total
        scaled[at, :] = (total * gain[...]).astype(BF16)

    x_copies, a_copies, r_copies, s_copies = {}, {}, {}, {}
    y_copies, e_copies, z_copies = {}, {}, {}

    def spread(i):
        if i == n_sp:
            gathered = x_tail[0].astype(F32)
            for j in range(1, n_sp):
                x_copies[j, "tail"].wait_recv()
                gathered = gathered + x_tail[j].astype(F32)
            x_all[block(i), feats(0)] = gathered.astype(BF16)
        elif i:
            x_copies[i].wait_recv()
        part = x_all.at[block(i), feats(0)]
        for q in (1, 2):
            a_copies[q, i] = start(
                remote(part, part, a_send.at[q, i], a_recv.at[q, i], me, tp_peer[q])
            )

    def relay(i):
        for q in (1, 2):
            whole = x_all.at[block(i), feats(q)]
            remote(whole, whole, a_send.at[q, i], a_recv.at[q, i], me, tp_peer[q]).wait_recv()
            part = x_all.at[block(i), feats(q, half, (q - 1) * half)]
            r_copies[q, i] = start(
                remote(part, part, r_send.at[q, i], r_recv.at[q, i], me, tp_peer[3 - q])
            )

    def await_block(i):
        for q in (1, 2):
            part = x_all.at[block(i), feats(3, half, (q - 1) * half)]
            remote(part, part, r_send.at[q, i], r_recv.at[q, i], me, tp_peer[3 - q]).wait_recv()

    def send_picked(i):
        picked = dot(pick_st[i * cap : (i + 1) * cap, :], scaled[...]).astype(BF16)
        if i:
            x_out[i] = picked
            x_copies[i] = start(
                remote(
                    x_out.at[i, 0:base, :], x_all.at[block(i), feats(0)], x_send.at[i],
                    x_recv.at[i], sp_peer[i], tp,
                )
            )
            x_copies[i, "tail"] = start(
                remote(
                    x_out.at[i, base:cap, :], x_tail.at[i], g_send.at[i], g_recv.at[i],
                    sp_peer[i], tp,
                )
            )
        else:
            x_all[block(0), feats(0)] = picked[0:base]
            x_tail[0] = picked[base:cap]

    n_copies = {}

    def send_sums(_):
        total = after[...]
        square_sum = jnp.sum(total * total, axis=1, keepdims=True)
        n_out[...] = jnp.transpose(jnp.broadcast_to(square_sum, (rows, 128)))[0:8, :]
        for q in (3, 1, 2):
            n_copies[q] = start(
                remote(n_out, n_in.at[q], n_send.at[q], n_recv.at[q], me, tp_peer[q])
            )

    def send_scales(_):
        sum_rows = n_out[...]
        for q in (1, 2, 3):
            n_copies[q].wait_recv()
            sum_rows = sum_rows + n_in[q]
        scale_c = jnp.transpose(lax.rsqrt(sum_rows / features + norm_eps))[:, 0:1]
        lane = lax.broadcasted_iota(jnp.int32, (rows, 128), 1)
        for i in range(n_sp):
            spot = jnp.where(lane < base, lane + i * base, lane - base + full + i * extra)
            here = (spot == slots_c[0]) | (spot == slots_c[1])
            row = jnp.sum(jnp.where(here, scale_c, 0.0), axis=0, keepdims=True)
            tile = jnp.broadcast_to(row, (8, 128))
            if i:
                s_out[i] = tile
                s_copies[i] = start(
                    remote(s_out.at[i], s_in.at[i], s_send.at[i], s_recv.at[i], sp_peer[i], tp)
                )
            else:
                s_in[0] = tile

    tile = min(256, hidden)
    scaled_by = {0}

    def scales_of(i):
        if i not in scaled_by:
            s_copies[i].wait_recv()
            scaled_by.add(i)
        return s_in[i]

    def size_of(g):
        return pair + extra if g == groups - 1 else pair

    def gate_up(g):
        members = [2 * g, 2 * g + 1]
        scale = [jnp.transpose(scales_of(i))[0:base, 0:1] for i in members]
        if g == groups - 1:
            tails = sum(scales_of(i) for i in range(n_sp))
            scale.append(jnp.transpose(tails)[base:cap, 0:1])
            members.append(n_sp)
        scale = jnp.concatenate(scale, axis=0)
        for i in members:
            await_block(i)
        span = pl.ds(g * pair, size_of(g))
        used = pl.ds(0, size_of(g))

        def hidden_tile(t, carry):
            at = pl.ds(pl.multiple_of(t * tile, 128), tile)
            gate = dot(x_all[span, :], wg[:, at]) * scale
            up = dot(x_all[span, :], wu[:, at]) * scale
            act[used, at] = (gate / (1.0 + jnp.exp(-gate)) * up).astype(BF16)
            return carry

        lax.fori_loop(0, hidden // tile, hidden_tile, 0)

    def down(g):
        span = pl.ds(g * pair, size_of(g))
        used = pl.ds(0, size_of(g))
        diag = dot(act[used, :], wd[:, feats(3)]).astype(BF16)
        y_out[0, 0, span, :] = diag[:, :half]
        y_out[1, 0, span, :] = diag[:, half:]
        by_x = dot(act[used, :], wd[:, feats(1)]).astype(BF16)
        y_out[0, 1, span, :] = by_x[:, :half]
        y_keep[1, span, :] = by_x[:, half:]
        by_y = dot(act[used, :], wd[:, feats(2)]).astype(BF16)
        y_out[1, 1, span, :] = by_y[:, half:]
        y_keep[0, span, :] = by_y[:, :half]
        y_own[span, :] = dot(act[used, :], wd[:, feats(0)]).astype(BF16)

    def send_parts(i):
        for h in range(2):
            at = (h, slice(None), block(i), slice(None))
            y_copies[h, i] = start(
                remote(
                    y_out.at[at], y_in.at[at], y_send.at[h, i], y_recv.at[h, i], me, tp_peer[1 + h]
                )
            )

    def pass_on(i):
        for h in range(2):
            y_copies[h, i].wait_recv()
            both = y_in[h, 0, block(i), :].astype(F32) + y_keep[h, block(i), :].astype(F32)
            y_fwd[h, block(i), :] = both.astype(BF16)
            at = (h, block(i), slice(None))
            e_copies[h, i] = start(
                remote(
                    y_fwd.at[at], y_last.at[at], e_send.at[h, i], e_recv.at[h, i], me, tp_peer[2 - h]
                )
            )

    def finish(i):
        for h in range(2):
            e_copies[h, i].wait_recv()
            at = slice(h * half, (h + 1) * half)
            piece = y_own[block(i), at].astype(F32) + y_in[h, 1, block(i), :].astype(F32)
            piece = (piece + y_last[h, block(i), :].astype(F32)).astype(BF16)
            if i == n_sp:
                z_tail[:, at] = piece
                z_in[full : full + extra, at] = piece
            elif i:
                z_out[i, :, at] = piece
            else:
                z_in[0:base, at] = piece
        if i == n_sp:
            for j in range(1, n_sp):
                z_copies[j, "tail"] = start(
                    remote(
                        z_tail, z_in.at[pl.ds(full + j * extra, extra), :], h_send.at[j],
                        h_recv.at[j], sp_peer[j], tp,
                    )
                )
        elif i:
            z_copies[i] = start(
                remote(
                    z_out.at[i], z_in.at[block(i), :], z_send.at[i], z_recv.at[i], sp_peer[i], tp
                )
            )

    def mixed(g):
        for i in (2 * g, 2 * g + 1):
            if i:
                z_copies[i].wait_recv()
        size = pair
        if g == groups - 1:
            for j in range(1, n_sp):
                z_copies[j, "tail"].wait_recv()
            size = pair + n_sp * extra
        total = after[...]
        for k in range(TOPK):
            gathered = dot(mixers[g, k, :, 0:size], z_in[g * pair : g * pair + size, :])
            total = total + gathered * mix_c[k]
        return total

    def mix(g):
        after[...] = mixed(g)

    def mix_last(_):
        out[...] = mixed(0)

    def await_weights(_):
        for load in loads:
            load.wait()

    steps = {
        "X": send_picked, "S": spread, "R": relay, "N": send_scales, "W": await_weights,
        "Q": send_sums, "G": gate_up, "D": down, "Y": send_parts, "P": pass_on, "F": finish, "M": mix, "E": mix_last,
    }
    for step in order:
        steps[step[0]](int(step[1:] or 0))

    for copy in sent:
        copy.wait_send()


def turn_table(tokens):
    quarter = E // 4
    frequency = (rope_base ** (-np.arange(quarter) / quarter)).astype(np.float32)
    grid_rows = tokens // GRID_W

    def lanes_of(count, first):
        angles = np.arange(count, dtype=np.float32)[:, None] * frequency[None, :]
        blank = np.zeros((count, 2 * quarter), np.float32)
        cosine = np.concatenate([np.cos(angles)] * 2, axis=1)
        sines = np.concatenate([-np.sin(angles), np.sin(angles)], axis=1)
        both = []
        for part in (cosine, sines):
            head = [part, blank] if first else [blank, part]
            both += head * 2
        return np.concatenate(both, axis=1)

    return np.concatenate([lanes_of(grid_rows, True), lanes_of(GRID_W, False)], axis=0)


ORDER = (
    "X4", "X0", "S0", "X2", "X1", "S1", "Q", "R0", "X5", "S2", "X3", "S4", "X6", "R1", "S5", "N",
    "W", "S3", "R4", "X7", "R5", "S6", "R2", "G0", "D0", "S7", "R3", "S8", "G2", "D2", "R6", "Y5",
    "Y4", "R7", "R8", "G1", "D1", "P5", "P4", "Y2", "Y3", "G3", "D3", "F5", "F4", "P2", "Y7",
    "Y8", "Y6", "F2", "P3", "P7", "P8", "P6", "Y1", "Y0", "F7", "F8", "F3", "M2", "P1", "F6",
    "P0", "F1", "M1", "M3", "F0", "E",
)


def fused_shards(
    n_sp,
    n_tp,
    query_heads,
    key_heads,
    value_heads,
    q_gain,
    k_gain,
    out_weight,
    residual,
    norm_gain,
    routes,
    route_weights,
    w_gate,
    w_up,
    w_down,
):
    rows, cols = residual.shape
    width = query_heads.shape[1]
    heads = width // E
    hidden = w_gate.shape[2]
    features = cols * n_tp
    cap = 5 * rows * TOPK // (4 * n_sp) + 1
    tail = cap % ROW_TILE or ROW_TILE
    base = cap - tail
    extra = -(-n_sp * tail // ROW_TILE) * ROW_TILE
    cap = base + extra
    slots = n_sp * base + extra
    pair = 2 * base
    half = cols // 2
    chunks = 8
    chunk = rows // chunks
    dma = pltpu.SemaphoreType.DMA
    vmem = pl.BlockSpec(memory_space=VMEM)
    hbm = pl.BlockSpec(memory_space=pl.ANY)
    table = jnp.asarray(turn_table(n_sp * rows))
    small = (
        query_heads, key_heads, value_heads, q_gain.reshape(1, E), k_gain.reshape(1, E), table,
        residual, norm_gain.reshape(1, cols), routes.T, route_weights.T,
    )
    total = pl.pallas_call(
        functools.partial(fused_kernel, n_sp, n_tp, base, tail, chunks, ORDER),
        out_shape=jax.ShapeDtypeStruct((rows, cols), F32),
        in_specs=[hbm] * (4 + len(small)),
        out_specs=vmem,
        scratch_shapes=[VMEM(array.shape, array.dtype) for array in small] + [
            VMEM((features, hidden), BF16),
            VMEM((features, hidden), BF16),
            VMEM((hidden, features), BF16),
            VMEM((n_tp, width, cols), BF16),
            VMEM((rows, 2 * E), BF16),
            VMEM((n_sp, rows, 2 * E), BF16),
            VMEM((heads * rows, 2 * E), BF16),
            VMEM((heads * rows, n_sp * rows), F32),
            VMEM((heads * rows, 128), F32),
            VMEM((heads * chunk, n_sp * rows), BF16),
            VMEM((heads * chunk, 128), F32),
            VMEM((n_tp, chunks, chunk, width), BF16),
            VMEM((n_sp * cap, rows), BF16),
            VMEM((n_sp // 2, TOPK, rows, pair + n_sp * extra), BF16),
            VMEM((rows, cols), BF16),
            VMEM((rows, cols), F32),
            VMEM((8, rows), F32),
            VMEM((n_tp, 8, rows), F32),
            VMEM((n_sp, 8, 128), F32),
            VMEM((n_sp, 8, 128), F32),
            VMEM((n_sp, cap, cols), BF16),
            VMEM((n_sp, extra, cols), BF16),
            VMEM((slots, features), BF16),
            VMEM((pair + extra, hidden), BF16),
            VMEM((2, 2, slots, half), BF16),
            VMEM((2, 2, slots, half), BF16),
            VMEM((slots, cols), BF16),
            VMEM((2, slots, half), BF16),
            VMEM((2, slots, half), BF16),
            VMEM((2, slots, half), BF16),
            VMEM((n_sp, base, cols), BF16),
            VMEM((extra, cols), BF16),
            VMEM((n_sp * cap, cols), BF16),
            dma((len(small),)),
            dma((4,)),
            dma((n_tp,)), dma((n_tp,)),
            dma((n_tp,)), dma((n_tp,)),
            dma((n_sp,)), dma((n_sp,)),
            dma((n_tp, chunks)), dma((n_tp, chunks)),
            dma((n_tp,)), dma((n_tp,)),
            dma((n_sp,)), dma((n_sp,)),
            dma((n_sp,)), dma((n_sp,)),
            dma((n_sp,)), dma((n_sp,)),
            dma((3, n_sp + 1)), dma((3, n_sp + 1)),
            dma((3, n_sp + 1)), dma((3, n_sp + 1)),
            dma((2, n_sp + 1)), dma((2, n_sp + 1)),
            dma((2, n_sp + 1)), dma((2, n_sp + 1)),
            dma((n_sp,)), dma((n_sp,)),
            dma((n_sp,)), dma((n_sp,)),
        ],
        compiler_params=pltpu.CompilerParams(
            collective_id=2, has_side_effects=True, vmem_limit_bytes=60 * 1024 * 1024
        ),
    )(out_weight, w_gate[0], w_up[0], w_down[0], *small)
    return total.astype(BF16)


def solution(mesh):
    n_sp, n_tp = mesh.shape["sp"], mesh.shape["tp"]
    local = fused_shards if n_tp == 4 and n_sp == 8 else shards
    return jax.shard_map(
        functools.partial(local, n_sp, n_tp),
        mesh=mesh,
        in_specs=(
            P("sp", "tp"),
            P("sp", None),
            P("sp", None),
            P(),
            P(),
            P("tp", None),
            P("sp", "tp"),
            P("tp"),
            P("sp", None),
            P("sp", None),
            P("sp", None, "tp"),
            P("sp", None, "tp"),
            P("sp", "tp", None),
        ),
        out_specs=P("sp", "tp"),
        check_vma=False,
    )
```
